512 devices in a mesh: sp: 128 (over z, y, core), tp: 4 (over x).
Axes of the slice: x: 4, y: 8, z: 8, core: 2. Of those that a mesh axis runs over, the one named last changes fastest.
Arguments:
- tokens: bfloat16 [16384, 2048], P(('sp', 'tp')), may hold values from -6 to 6
- doc_lengths: int32 [16], replicated, may hold values from 1 to 10240, 16384 in all
- query_down: bfloat16 [2048, 512], replicated, may hold values from -0.125 to 0.125
- latent_down: bfloat16 [2048, 256], replicated, may hold values from -0.125 to 0.125
- rope_down: bfloat16 [2048, 32], replicated, may hold values from -0.125 to 0.125
- query_latent_gain: float32 [512], replicated, may hold values from 0.1 to 1.9
- latent_gain: float32 [256], replicated, may hold values from 0.1 to 1.9
- query_up: bfloat16 [512, 768], P(None, 'tp'), may hold values from -0.25 to 0.25
- key_up: bfloat16 [256, 512], P(None, 'tp'), may hold values from -0.375 to 0.375
- value_up: bfloat16 [256, 512], P(None, 'tp'), may hold values from -0.375 to 0.375
- query_gain: float32 [96], replicated, may hold values from 0.5 to 15
- key_gain: float32 [96], replicated, may hold values from 0.5 to 15
- output_gain: float32 [512], replicated, may hold values from 0.1 to 1.9
- output_weight: bfloat16 [512, 2048], P(None, 'tp'), may hold values from -0.25 to 0.25
Outputs:
- layer_output: bfloat16 [16384, 2048], P('sp', 'tp')
- log_totals: float32 [8, 16384], P('tp', 'sp')
The draws below stay inside these ranges and needn't reach their ends.
Inputs may be any that keep to these rules, and one draw needn't show every extreme that they name: `doc_lengths`: the lengths sum to 16384; the longest is exactly 10240.
All inputs are finite; a program needn't handle non-finite values.
Results may differ from the reference program's by a relative error of at most 0.019.
The reference program's roundings to bfloat16 on the way count: a program that leaves them out, or rounds other values in their place, can miss the bound.
Values may be sent and summed in bfloat16 or wider, within the bound.
A program may use at most 64 MiB of HBM per device.

```python
import math
import jax
import jax.numpy as jnp
import numpy as np
from jax import lax

D = 2048
QR = 512
KVR = 256
H = 8
NOPE = 64
ROPE = 32
VD = 64
NDOC = 16
SEQ = 16384


def gain_table(key, salt_value):
    gains_out = jax.random.uniform(jax.random.fold_in(key, salt_value), (NOPE + ROPE,), jnp.float32, 0.5, 1.5)
    return gains_out


def draw_query_gain(key, part):
    return gain_table(key, 101)


def draw_key_gain(key, part):
    return gain_table(key, 202)


def block_scale(key, dims, split, least, top_value):
    gain = 1.0
    for position, shards_of in split:
        draws = jax.random.uniform(jax.random.fold_in(jax.random.fold_in(key, 6), position), (shards_of,), jnp.float32, least / len(split), top_value / len(split))
        gain = gain * jnp.repeat(jnp.exp(draws), dims[position] // shards_of).reshape((-1,) + (1,) * (len(dims) - 1 - position))
    return gain


def length_profile(amount, total, most, lean):
    weights = [(1 << 20) // math.isqrt(standing ** lean) + 1 for standing in range(2, amount + 1)]
    rest, given = total - most - (amount - 1), [1] * (amount - 1)
    while rest > 0:
        candidates = [i for i in range(amount - 1) if given[i] < most]
        mass, remaining = sum([weights[i] for i in candidates]), rest
        for i in candidates:
            addition = min(most - given[i], max(1, remaining * weights[i] // mass), rest)
            given[i] = given[i] + addition
            rest = rest - addition
    return np.array([most] + given)


def uneven(own_key, amount, total, most, lean):
    if amount == 2:
        one = jax.random.randint(own_key, (), max(1, total - most), min(most, total - 1) + 1)
        return jnp.stack([one, total - one])
    tallies = jnp.asarray(length_profile(amount, total, most, lean), jnp.int32)
    pairs = (amount - 1) // 2
    giver, taker = tallies[1:1 + 2 * pairs:2], tallies[2:2 + 2 * pairs:2]
    margin = jnp.minimum(giver - 1, most - taker)
    shifted = jax.random.randint(jax.random.fold_in(own_key, 1), (pairs,), 0, 1 << 20) % (margin + 1)
    tallies = tallies.at[1:1 + 2 * pairs:2].set(giver - shifted).at[2:2 + 2 * pairs:2].set(taker + shifted)
    return tallies[jax.random.permutation(jax.random.fold_in(own_key, 2), amount)]


def normal_values(own_key, shape, scale, limit, shards=(), kind=jnp.bfloat16):
    level = block_scale(own_key, shape, shards, -0.22, 0.18) if shards else 1.0
    values = jax.random.normal(own_key, shape, jnp.float32) * scale * level
    return jnp.minimum(jnp.maximum(values, -limit), limit).astype(kind)


def setup_inputs(seed: int = 0) -> dict:
    keys = jax.random.split(jax.random.key(seed), 15)
    return {
        "tokens": normal_values(keys[0], (SEQ, D), 1.0, 6.0, ((0, 512),)),
        "doc_lengths": uneven(keys[1], NDOC, SEQ, SEQ * 5 // 8, 2).astype(jnp.int32),
        "query_down": normal_values(keys[2], (D, QR), D ** -0.5, 0.125),
        "latent_down": normal_values(keys[3], (D, KVR), D ** -0.5, 0.125),
        "rope_down": normal_values(keys[4], (D, ROPE), D ** -0.5, 0.125),
        "query_latent_gain": jnp.clip(1.0 + 0.18 * jax.random.normal(keys[5], (QR,), jnp.float32), 0.1, 1.9),
        "latent_gain": jnp.clip(1.0 + 0.18 * jax.random.normal(keys[6], (KVR,), jnp.float32), 0.1, 1.9),
        "query_up": normal_values(keys[7], (QR, H * (NOPE + ROPE)), QR ** -0.5, 0.25, ((1, 4),)),
        "key_up": normal_values(keys[8], (KVR, H * NOPE), KVR ** -0.5, 0.375, ((1, 4),)),
        "value_up": normal_values(keys[9], (KVR, H * VD), KVR ** -0.5, 0.375, ((1, 4),)),
        "query_gain": draw_query_gain(jax.random.fold_in(keys[14], 71), 0),
        "key_gain": draw_key_gain(jax.random.fold_in(keys[14], 71), 0),
        "output_gain": jnp.clip(1.0 + 0.18 * jax.random.normal(keys[12], (H * VD,), jnp.float32), 0.1, 1.9),
        "output_weight": normal_values(keys[13], (H * VD, D), (H * VD) ** -0.5, 0.25, ((1, 4),)),
    }


EPS = 1e-06
THETA = 10000.0
NEG = -1e+30

def norm_rows(matrix, scaling):
    mean_square = lax.optimization_barrier(jnp.mean(matrix * matrix, axis=-1, keepdims=True))
    return matrix * lax.rsqrt(mean_square + EPS) * scaling

def rotate(matrix, places):
    half_width = matrix.shape[-1] // 2
    inverse = THETA ** (-jnp.arange(half_width, dtype=jnp.float32) / half_width)
    angles = places.astype(jnp.float32)[:, None, None] * inverse
    cosine = jnp.cos(angles)
    sine_part = jnp.sin(angles)
    leading = matrix[..., :half_width]
    trailing = matrix[..., half_width:]
    return jnp.concatenate([leading * cosine - trailing * sine_part, trailing * cosine + leading * sine_part], axis=-1)

def doc_index(places, doc_ends):
    return lax.optimization_barrier(jnp.sum((places[:, None] >= doc_ends[None, :]).astype(jnp.int32), axis=1)).astype(jnp.int32)

def head_keys(latent_rows, rope_rows, places, key_up, value_up, key_gain):
    row_count = latent_rows.shape[0]
    head_count = key_up.shape[1] // NOPE
    plain_part = jnp.dot(latent_rows, key_up, preferred_element_type=jnp.float32).reshape(row_count, head_count, NOPE)
    shared_part = jnp.broadcast_to(rope_rows.astype(jnp.float32)[:, None, :], (row_count, head_count, ROPE))
    joined = norm_rows(jnp.concatenate([plain_part, shared_part], axis=-1), key_gain)
    key_block = jnp.concatenate([joined[..., :NOPE], rotate(joined[..., NOPE:], places)], axis=-1).astype(jnp.bfloat16)
    value_block = jnp.dot(latent_rows, value_up, preferred_element_type=jnp.float32).astype(jnp.bfloat16)
    return (key_block, value_block.reshape(row_count, head_count, VD))

def reference(tokens, doc_lengths, query_down, latent_down, rope_down, query_latent_gain, latent_gain, query_up, key_up, value_up, query_gain, key_gain, output_gain, output_weight):
    head_width = NOPE + ROPE
    query_latent = norm_rows(jnp.dot(tokens, query_down, preferred_element_type=jnp.float32), query_latent_gain).astype(jnp.bfloat16)
    key_latent = norm_rows(jnp.dot(tokens, latent_down, preferred_element_type=jnp.float32), latent_gain).astype(jnp.bfloat16)
    rope_key = jnp.dot(tokens, rope_down, preferred_element_type=jnp.float32).astype(jnp.bfloat16)
    places = jnp.arange(SEQ, dtype=jnp.int32)
    doc_ends = jnp.cumsum(doc_lengths).astype(jnp.int32)
    docs = doc_index(places, doc_ends)
    query_raw = jnp.dot(query_latent, query_up, preferred_element_type=jnp.float32).reshape(SEQ, H, head_width)
    query_raw = norm_rows(query_raw, query_gain)
    queries = jnp.concatenate([query_raw[..., :NOPE], rotate(query_raw[..., NOPE:], places)], axis=-1).astype(jnp.bfloat16)
    key_block, value_block = head_keys(key_latent, rope_key, places, key_up, value_up, key_gain)
    keys_wide = key_block.astype(jnp.float32)
    values_wide = value_block.astype(jnp.float32)
    block_rows = math.gcd(SEQ, 512)
    block_count = SEQ // block_rows
    score_scale = head_width ** (-0.5)

    def one_block(block_index):
        begin_at = (block_index * block_rows).astype(jnp.int32)
        query_part = lax.dynamic_slice_in_dim(queries, begin_at, block_rows, 0).astype(jnp.float32)
        query_docs = lax.dynamic_slice_in_dim(docs, begin_at, block_rows, 0)
        scores = jnp.einsum('qhd,khd->hqk', query_part, keys_wide) * score_scale
        allowed = (query_docs[:, None] == docs[None, :])[None]
        scores = jnp.where(allowed, scores, NEG)
        row_top = lax.optimization_barrier(jnp.max(scores, axis=-1))
        expd_part = jnp.where(allowed, jnp.exp(scores - row_top[..., None]), 0.0)
        row_total = lax.optimization_barrier(jnp.sum(expd_part, axis=-1))
        weights = lax.optimization_barrier(expd_part.astype(jnp.bfloat16)).astype(jnp.float32)
        weighted = jnp.einsum('hqk,khd->qhd', weights, values_wide)
        head_out = (weighted / jnp.transpose(row_total)[:, :, None]).astype(jnp.bfloat16)
        return (head_out, row_top + jnp.log(row_total))
    head_blocks, log_blocks = lax.map(one_block, jnp.arange(block_count, dtype=jnp.int32))
    head_out = head_blocks.reshape(SEQ, H * VD)
    log_totals = jnp.transpose(log_blocks, (1, 0, 2)).reshape(H, SEQ)
    normed = norm_rows(head_out.astype(jnp.float32), output_gain).astype(jnp.bfloat16)
    layer_output = jnp.dot(normed, output_weight, preferred_element_type=jnp.float32).astype(jnp.bfloat16)
    return (layer_output, log_totals)
```

```python
import functools

import jax
import jax.numpy as jnp
import numpy as np
from jax import lax
from jax.experimental import pallas as pl
from jax.experimental.pallas import tpu as pltpu
from jax.sharding import PartitionSpec as P

NOPE = 64
ROPE = 32
VD = 64
NDOC = 16
WIDTH = NOPE + ROPE
EPS = 1e-06
THETA = 10000.0
APART = -float(2**20)
SCALE = WIDTH**-0.5
LOG2E = 1.4426950408889634
F32 = jnp.float32
BF16 = jnp.bfloat16
MESH = pl.DeviceIdType.MESH
DOC_LANE = 64


def split_of(count):
    return {128: (8, 8, 2), 8: (2, 2, 2), 16: (2, 4, 2)}[count]


def tables(blocks):
    half = ROPE // 2
    inverse = THETA ** (-(np.arange(128) % half).astype(np.float64) / half)
    fine = np.arange(128)[:, None] * inverse[None]
    coarse = (np.arange(blocks) * 128)[:, None] * inverse[None]
    fine = np.stack([np.cos(fine), np.sin(fine)]).astype(np.float32)
    coarse = np.stack([np.cos(coarse), np.sin(coarse)]).astype(np.float32)
    return fine, coarse


def query_columns():
    out = np.zeros((2 * WIDTH, 384), np.float32)
    for j in range(128):
        out[(j // 64) * WIDTH + j % 64, j] = 1
        head, entry = (j % 64) // 32, j % 32
        out[head * WIDTH + NOPE + entry, 128 + j] = 1
        out[head * WIDTH + NOPE + (entry + 16) % 32, 256 + j] = 1
    return out


def rope_spread():
    out = np.zeros((128, 1024), np.float32)
    for g in range(4):
        for j in range(64):
            out[32 * g + j % 32, 256 * g + j] = 1
            out[32 * g + (j % 32 + 16) % 32, 256 * g + 128 + j] = 1
    return out


def sum_matrix(rope_lanes):
    out = np.zeros((256, 256), np.float32)
    for col in range(256):
        head = col // 64 if col < 128 else ((col - 128) // 32) % 2
        for i in range(128):
            out[i, col] = i // 64 == head
        for i in range(64):
            if rope_lanes == 32:
                out[128 + i, col] = i < 32
            else:
                out[128 + i, col] = i // 32 == head
    return out


def dot(a, b):
    return jnp.dot(a, b, preferred_element_type=F32)


def dot_t(a, b):
    return lax.dot_general(a, b, (((1,), (1,)), ((), ())), preferred_element_type=F32)


def lanes(rows, width=128):
    return lax.broadcasted_iota(jnp.int32, (rows, width), 1)


def rows_of(rows, width=128):
    return lax.broadcasted_iota(jnp.int32, (rows, width), 0)


def head_sums(squares, matrix):
    high = squares.astype(BF16)
    low = (squares - high.astype(F32)).astype(BF16)
    return dot(high, matrix) + dot(low, matrix)


def kernel(
    Z, Y, C, X,
    tok, doclen, qdown, ldown, rdown, qlgain, lgain, qup, kup, vup, gains, ogain, oweight,
    fine, coarse, qcols, spread, ksum, qsum,
    out, logs,
    qlbuf, klbuf, rkbuf, qbuf, kall, vtall, sbuf, pbuf, vupt, osend, lsend, orecv, lrecv, hobuf, bounds,
    ql_s, ql_r, kz_s, kz_r, kx_s, kx_r, kc_s, kc_r, qy_s, qy_r, o_s, o_r, ho_s, ho_r,
):
    s = lax.axis_index("sp")
    t = lax.axis_index("tp")
    z = s // (Y * C)
    y = lax.rem(s // C, Y)
    c = lax.rem(s, C)
    gz = Z * 32

    def at(zz, yy, cc):
        return (zz * Y + yy) * C + cc

    def zpeer(k):
        zz = lax.rem(z + k, Z)
        return zz, (at(zz, y, c), t)

    def ypeer(k):
        yy = lax.rem(y + k, Y)
        return yy, (at(z, yy, c), t)

    def xpeer(k):
        xx = lax.rem(t + k, X)
        return xx, (s, xx)

    other = (at(z, y, 1 - c), t)

    def remote(src, dst, ss, rs, who):
        return pltpu.make_async_remote_copy(
            src_ref=src, dst_ref=dst, send_sem=ss, recv_sem=rs, device_id=who, device_id_type=MESH
        )

    barrier = pltpu.get_barrier_semaphore()
    peers = [zpeer(k)[1] for k in range(1, Z)] + [ypeer(k)[1] for k in range(1, Y)]
    peers += [xpeer(k)[1] for k in range(1, X)] + [other]
    for who in peers:
        pl.semaphore_signal(barrier, inc=1, device_id=who, device_id_type=MESH)

    x = tok[...]
    qd = dot(x, qdown[...])
    qd = qd * lax.rsqrt(jnp.mean(qd * qd, axis=-1, keepdims=True) + EPS) * qlgain[...]
    qlbuf[t] = qd.astype(BF16)
    kd = dot(x, ldown[...])
    kd = kd * lax.rsqrt(jnp.mean(kd * kd, axis=-1, keepdims=True) + EPS) * lgain[...]
    klbuf[c, t, z] = kd.astype(BF16)
    rk = dot(x, rdown[...]).astype(BF16)
    four = (lanes(32) % 32 == rows_of(32)).astype(F32).astype(BF16)
    rk4 = dot(rk, four)
    group = lanes(8) // 32
    packed = jnp.where(group == 0, rk4[0:8], jnp.where(group == 1, rk4[8:16], jnp.where(group == 2, rk4[16:24], rk4[24:32])))
    rkbuf[c, t, z] = packed

    pl.semaphore_wait(barrier, len(peers))

    sends = []
    for k in range(1, X):
        _, who = xpeer(k)
        copy = remote(qlbuf.at[t], qlbuf.at[t], ql_s.at[k], ql_r.at[k], who)
        copy.start()
        sends.append(copy)
    for k in range(1, Z):
        _, who = zpeer(k)
        for n, buf in enumerate((klbuf, rkbuf)):
            copy = remote(buf.at[c, t, z], buf.at[c, t, z], kz_s.at[n, k], kz_r.at[n, k], who)
            copy.start()
            sends.append(copy)

    lane1 = lanes(1)
    starts = jnp.full((1, 128), 1 << 30, jnp.int32)
    ends = jnp.zeros((1, 128), jnp.int32)
    total = jnp.int32(0)
    for d in range(NDOC):
        starts = jnp.where(lane1 == DOC_LANE + d, total, starts)
        total = total + doclen[d]
        ends = jnp.where(lane1 == DOC_LANE + d, total, ends)
    bounds[0:1, :] = starts
    bounds[1:2, :] = ends
    qweight = dot(qup[...], qcols[...]).astype(BF16)
    vupt[...] = jnp.transpose(vup[...].astype(F32)).astype(BF16)

    def turn(block, first, count):
        cb = coarse[0, pl.ds(block, 1), :]
        sb = coarse[1, pl.ds(block, 1), :]
        cf = fine[0, pl.ds(first, count), :]
        sf = fine[1, pl.ds(first, count), :]
        return cb * cf - sb * sf, sb * cf + cb * sf

    for k in range(1, X):
        xx = lax.rem(t - k + X, X)
        remote(qlbuf.at[xx], qlbuf.at[xx], ql_s.at[k], ql_r.at[k], (s, xx)).wait_recv()
    ql = qlbuf[...].reshape(128, qlbuf.shape[2])
    qq = dot(ql, qweight)
    q0, q1, q2 = qq[:, 0:128], qq[:, 128:256], qq[:, 256:384]
    qs = head_sums(jnp.concatenate([q0 * q0, q1 * q1], axis=1), qsum[...])
    qs = lax.rsqrt(qs * (1.0 / WIDTH) + EPS)
    cosine, sine = turn(s, 0, 128)
    plain = q0 * qs[:, 0:128] * gains[0:1, :]
    rope = (q1 * gains[1:2, :] * cosine + q2 * gains[2:3, :] * sine) * qs[:, 128:256]
    qbuf[y, 0:128, :] = plain.astype(BF16)
    qbuf[y, 128:192, :] = jnp.where(lanes(64) < 64, rope[0:64], rope[64:128]).astype(BF16)
    for k in range(1, Y):
        _, who = ypeer(k)
        copy = remote(qbuf.at[y], qbuf.at[y], qy_s.at[k], qy_r.at[k], who)
        copy.start()
        sends.append(copy)

    for k in range(1, Z):
        zz = lax.rem(z - k + Z, Z)
        for n, buf in enumerate((klbuf, rkbuf)):
            slot = buf.at[c, t, zz]
            remote(slot, slot, kz_s.at[n, k], kz_r.at[n, k], (at(zz, y, c), t)).wait_recv()
    for k in range(1, X):
        _, who = xpeer(k)
        for n, buf in enumerate((klbuf, rkbuf)):
            copy = remote(buf.at[c, t], buf.at[c, t], kx_s.at[n, k], kx_r.at[n, k], who)
            copy.start()
            sends.append(copy)

    def to_core(k):
        xx = lax.rem(t - k + X, X)
        for n, buf in enumerate((klbuf, rkbuf)):
            slot = buf.at[c, xx]
            copy = remote(slot, slot, kc_s.at[n, k], kc_r.at[n, k], other)
            copy.start()
            sends.append(copy)

    def expand(cc, xx):
        kl = klbuf[cc, xx].reshape(gz, klbuf.shape[4])
        index = cc * X + xx
        vtall[index] = dot_t(vupt[...], kl).astype(BF16)
        raw = dot(kl, kup[...])
        spreaded = dot(rkbuf[cc, xx].reshape(Z * 8, 128).astype(BF16), spread[...])

        def rows_from(shift):
            return jnp.concatenate(
                [spreaded[8 * zz : 8 * zz + 8, 256 * g + shift : 256 * g + shift + 128] for zz in range(Z) for g in range(4)],
                axis=0,
            )

        r1, r2 = rows_from(0), rows_from(128)
        sums = head_sums(jnp.concatenate([raw * raw, r1 * r1], axis=1), ksum[...])
        sums = lax.rsqrt(sums * (1.0 / WIDTH) + EPS)
        kall[index, :, 0:128] = (raw * sums[:, 0:128] * gains[3:4, :]).astype(BF16)
        first = pl.multiple_of(xx * 32, 32)
        for zz in range(Z):
            block = at(zz, y, cc)
            cosine, sine = turn(block, first, 32)
            part = slice(zz * 32, zz * 32 + 32)
            turned = (r1[part] * gains[4:5, :] * cosine + r2[part] * gains[5:6, :] * sine) * sums[part, 128:256]
            place = block * 128 + first + rows_of(32)
            inside = (place >= bounds[0:1, :]) & (place < bounds[1:2, :])
            kall[index, part, 128:256] = jnp.where(inside, 1.0, turned).astype(BF16)

    to_core(0)
    expand(c, t)
    for k in range(1, X):
        xx = lax.rem(t - k + X, X)
        for n, buf in enumerate((klbuf, rkbuf)):
            slot = buf.at[c, xx]
            remote(slot, slot, kx_s.at[n, k], kx_r.at[n, k], (s, xx)).wait_recv()
        to_core(k)
        expand(c, xx)
    for k in range(X):
        xx = lax.rem(t - k + X, X)
        for n, buf in enumerate((klbuf, rkbuf)):
            slot = buf.at[1 - c, xx]
            remote(slot, slot, kc_s.at[n, k], kc_r.at[n, k], other).wait_recv()
        expand(1 - c, xx)

    groups = C * X

    def attend(yy):
        block = at(z, yy, c)
        qplain = qbuf[yy, 0:128, :].astype(F32)
        qrope = qbuf[yy, 128:192, :].astype(F32)
        qrope = jnp.concatenate([qrope, pltpu.roll(qrope, 64, 1)], axis=0)
        place = block * 128 + rows_of(128)
        inside = (place >= bounds[0:1, :]) & (place < bounds[1:2, :])
        lane = lanes(128)
        apart = jnp.where((lane >= DOC_LANE) & (lane < DOC_LANE + NDOC) & jnp.logical_not(inside), APART, 0.0)
        both = []
        for h in range(2):
            left = jnp.where(lane // 64 == h, qplain, 0.0)
            right = jnp.where(lane // 32 == h, qrope, apart)
            both.append(jnp.concatenate([left, right], axis=1))
        queries = jnp.concatenate(both, axis=0).astype(BF16)
        top = None
        for g in range(groups):
            scores = dot_t(kall[g], queries)
            sbuf[g] = scores
            most = jnp.max(scores, axis=0, keepdims=True)
            top = most if top is None else jnp.maximum(top, most)
        count = None
        acc = None
        for g in range(groups):
            weights = jnp.exp2((sbuf[g] - top) * (SCALE * LOG2E))
            added = jnp.sum(weights, axis=0, keepdims=True)
            count = added if count is None else count + added
            update = dot(vtall[g], weights.astype(BF16))
            acc = update if acc is None else acc + update
        log = top * SCALE + jnp.log(count)
        lsend[yy] = jnp.where(rows_of(8) == 0, log[:, 0:128], log[:, 128:256])
        inv = 1.0 / count
        osend[yy, 0:64, :] = (acc[0:64, 0:128] * inv[:, 0:128]).astype(BF16)
        osend[yy, 64:128, :] = (acc[64:128, 128:256] * inv[:, 128:256]).astype(BF16)

    def step(i, carry):
        off = jnp.where(lax.rem(i, 2) == 1, (i + 1) // 2, Y - i // 2)
        k = lax.rem(off, Y)
        yy, who = ypeer(k)
        back = lax.rem(Y - k, Y)

        @pl.when(i > 0)
        def _():
            remote(qbuf.at[yy], qbuf.at[yy], qy_s.at[back], qy_r.at[back], who).wait_recv()

        attend(yy)

        @pl.when(i > 0)
        def _():
            remote(osend.at[yy], orecv.at[y], o_s.at[0, k], o_r.at[0, k], who).start()
            remote(lsend.at[yy], lrecv.at[y], o_s.at[1, k], o_r.at[1, k], who).start()

        return carry

    lax.fori_loop(0, Y, step, 0)

    orecv[y] = osend[y]
    lrecv[y] = lsend[y]
    for k in range(1, Y):
        yy = lax.rem(y - k + Y, Y)
        who = (at(z, yy, c), t)
        remote(osend.at[yy], orecv.at[yy], o_s.at[0, k], o_r.at[0, k], who).wait_recv()
        remote(lsend.at[yy], lrecv.at[yy], o_s.at[1, k], o_r.at[1, k], who).wait_recv()
    top = lrecv[0]
    for i in range(1, Y):
        top = jnp.maximum(top, lrecv[i])
    whole = jnp.zeros_like(top)
    acc0 = jnp.zeros((64, 128), F32)
    acc1 = jnp.zeros((64, 128), F32)
    for i in range(Y):
        weight = jnp.exp(lrecv[i] - top)
        whole = whole + weight
        acc0 = acc0 + weight[0:1] * orecv[i, 0:64, :].astype(F32)
        acc1 = acc1 + weight[1:2] * orecv[i, 64:128, :].astype(F32)
    logs[...] = (top + jnp.log(whole))[0:2]
    inv = 1.0 / whole
    heads = jnp.concatenate([acc0 * inv[0:1], acc1 * inv[1:2]], axis=0)
    hobuf[t] = jnp.transpose(heads).astype(BF16)
    for k in range(1, X):
        _, who = xpeer(k)
        copy = remote(hobuf.at[t], hobuf.at[t], ho_s.at[k], ho_r.at[k], who)
        copy.start()
        sends.append(copy)
    for k in range(1, Y):
        yy, who = ypeer(k)
        remote(osend.at[yy], orecv.at[y], o_s.at[0, k], o_r.at[0, k], who).wait_send()
        remote(lsend.at[yy], lrecv.at[y], o_s.at[1, k], o_r.at[1, k], who).wait_send()
    for k in range(1, X):
        xx = lax.rem(t - k + X, X)
        remote(hobuf.at[xx], hobuf.at[xx], ho_s.at[k], ho_r.at[k], (s, xx)).wait_recv()
    full = jnp.concatenate([hobuf[i].astype(F32) for i in range(X)], axis=1)
    normed = full * lax.rsqrt(jnp.mean(full * full, axis=-1, keepdims=True) + EPS) * ogain[...]
    out[...] = dot(normed.astype(BF16), oweight[...]).astype(BF16)
    for copy in sends:
        copy.wait_send()


def gain_rows(gain):
    plain = gain[:NOPE]
    a, b = gain[NOPE : NOPE + 16], gain[NOPE + 16 :]
    rope = jnp.concatenate([a, b])
    swapped = jnp.concatenate([-b, a])
    return [jnp.concatenate([plain] * 2), jnp.concatenate([rope] * 4), jnp.concatenate([swapped] * 4)]


def per_device(
    split, X,
    tokens, doc_lengths, query_down, latent_down, rope_down, query_latent_gain, latent_gain,
    query_up, key_up, value_up, query_gain, key_gain, output_gain, output_weight,
):
    Z, Y, C = split
    blocks = Z * Y * C
    rows = gain_rows(query_gain) + gain_rows(key_gain)
    gains = jnp.stack(rows + [jnp.zeros((128,), F32)] * 2)
    fine, coarse = tables(blocks)
    vm = pl.BlockSpec(memory_space=pltpu.VMEM)
    sm = pl.BlockSpec(memory_space=pltpu.SMEM)
    dma = pltpu.SemaphoreType.DMA
    gz = Z * 32
    groups = C * X
    QR, KVR = query_down.shape[1], latent_down.shape[1]
    const = lambda a: jnp.asarray(a, BF16)
    return pl.pallas_call(
        functools.partial(kernel, Z, Y, C, X),
        out_shape=(
            jax.ShapeDtypeStruct((128, output_weight.shape[1]), BF16),
            jax.ShapeDtypeStruct((2, 128), F32),
        ),
        in_specs=[vm, sm] + [vm] * 17,
        out_specs=(vm, vm),
        scratch_shapes=[
            pltpu.VMEM((X, 32, QR), BF16),
            pltpu.VMEM((C, X, Z, 32, KVR), BF16),
            pltpu.VMEM((C, X, Z, 8, 128), F32),
            pltpu.VMEM((Y, 192, 128), BF16),
            pltpu.VMEM((groups, gz, 256), BF16),
            pltpu.VMEM((groups, 128, gz), BF16),
            pltpu.VMEM((groups, gz, 256), F32),
            pltpu.VMEM((8, 128), F32),
            pltpu.VMEM((128, KVR), BF16),
            pltpu.VMEM((Y, 128, 128), BF16),
            pltpu.VMEM((Y, 8, 128), F32),
            pltpu.VMEM((Y, 128, 128), BF16),
            pltpu.VMEM((Y, 8, 128), F32),
            pltpu.VMEM((X, 128, 128), BF16),
            pltpu.VMEM((8, 128), jnp.int32),
            dma((X,)), dma((X,)),
            dma((2, Z)), dma((2, Z)),
            dma((2, X)), dma((2, X)),
            dma((2, X)), dma((2, X)),
            dma((Y,)), dma((Y,)),
            dma((2, Y)), dma((2, Y)),
            dma((X,)), dma((X,)),
        ],
        compiler_params=pltpu.CompilerParams(
            collective_id=0, has_side_effects=True, vmem_limit_bytes=48 * 2**20
        ),
    )(
        tokens, doc_lengths, query_down, latent_down, rope_down,
        query_latent_gain.reshape(1, -1), latent_gain.reshape(1, -1),
        query_up, key_up, value_up, gains, output_gain.reshape(1, -1), output_weight,
        jnp.asarray(fine), jnp.asarray(coarse), const(query_columns()), const(rope_spread()),
        const(sum_matrix(32)), const(sum_matrix(64)),
    )


def solution(mesh):
    split = split_of(mesh.shape["sp"])
    return jax.shard_map(
        functools.partial(per_device, split, mesh.shape["tp"]),
        mesh=mesh,
        in_specs=(
            P(("sp", "tp"), None),
            P(), P(), P(), P(), P(), P(),
            P(None, "tp"), P(None, "tp"), P(None, "tp"),
            P(), P(), P(),
            P(None, "tp"),
        ),
        out_specs=(P("sp", "tp"), P("tp", "sp")),
        check_vma=False,
    )
```

```python
import functools

import jax
import jax.numpy as jnp
import numpy as np
from jax import lax
from jax.experimental import pallas as pl
from jax.experimental.pallas import tpu as pltpu
from jax.sharding import PartitionSpec as P

NOPE = 64
ROPE = 32
VD = 64
NDOC = 16
WIDTH = NOPE + ROPE
EPS = 1e-06
THETA = 10000.0
APART = -float(2**20)
SCALE = WIDTH**-0.5
LOG2E = 1.4426950408889634
F32 = jnp.float32
BF16 = jnp.bfloat16
MESH = pl.DeviceIdType.MESH
DOC_LANE = 64


def split_of(count):
    return {128: (8, 8, 2), 8: (2, 2, 2), 16: (2, 4, 2)}[count]


def tables(blocks):
    half = ROPE // 2
    inverse = THETA ** (-(np.arange(128) % half).astype(np.float64) / half)
    fine = np.arange(128)[:, None] * inverse[None]
    coarse = (np.arange(blocks) * 128)[:, None] * inverse[None]
    fine = np.stack([np.cos(fine), np.sin(fine)]).astype(np.float32)
    coarse = np.stack([np.cos(coarse), np.sin(coarse)]).astype(np.float32)
    return fine, coarse


def query_columns():
    out = np.zeros((2 * WIDTH, 384), np.float32)
    for j in range(128):
        out[(j // 64) * WIDTH + j % 64, j] = 1
        head, entry = (j % 64) // 32, j % 32
        out[head * WIDTH + NOPE + entry, 128 + j] = 1
        out[head * WIDTH + NOPE + (entry + 16) % 32, 256 + j] = 1
    return out


def rope_spread():
    out = np.zeros((128, 1024), np.float32)
    for g in range(4):
        for j in range(64):
            out[32 * g + j % 32, 256 * g + j] = 1
            out[32 * g + (j % 32 + 16) % 32, 256 * g + 128 + j] = 1
    return out


def sum_matrix(rope_lanes):
    out = np.zeros((256, 256), np.float32)
    for col in range(256):
        head = col // 64 if col < 128 else ((col - 128) // 32) % 2
        for i in range(128):
            out[i, col] = i // 64 == head
        for i in range(64):
            if rope_lanes == 32:
                out[128 + i, col] = i < 32
            else:
                out[128 + i, col] = i // 32 == head
    return out


def dot(a, b):
    return jnp.dot(a, b, preferred_element_type=F32)


def dot_t(a, b):
    return lax.dot_general(a, b, (((1,), (1,)), ((), ())), preferred_element_type=F32)


def lanes(rows, width=128):
    return lax.broadcasted_iota(jnp.int32, (rows, width), 1)


def rows_of(rows, width=128):
    return lax.broadcasted_iota(jnp.int32, (rows, width), 0)


def head_sums(squares, matrix):
    high = squares.astype(BF16)
    low = (squares - high.astype(F32)).astype(BF16)
    return dot(high, matrix) + dot(low, matrix)


def offsets(count):
    return [(i + 1) // 2 if i % 2 else (count - i // 2) % count for i in range(count)]


def gain_columns():
    out = np.zeros((WIDTH, 384), np.float32)
    for j in range(128):
        entry = j % 32
        out[j % 64, j] = 1
        out[NOPE + entry, 128 + j] = 1
        out[NOPE + (entry + 16) % 32, 256 + j] = -1 if entry < 16 else 1
    return out


def kernel(
    Z, Y, C, X, batches,
    tok_h, doclen, qdown_h, ldown_h, rdown_h, qlgain_h, lgain_h, qup_h, kup_h, vup_h, qgain_h, kgain_h, ogain_h, oweight_h,
    fine_h, coarse_h, qcols_h, spread_h, ksum_h, qsum_h, gcols_h,
    out, logs,
    tok, qdown, ldown, rdown, qlgain, lgain, qup, kup, vup, qgain, kgain, ogain, oweight,
    fine, coarse, qcols, spread, ksum, qsum, gcols,
    qlbuf, klbuf, rkbuf, qbuf, kall, vtall, sbuf, vupt, osend, lsend, orecv, lrecv, hobuf, bounds, gains,
    in_s, ql_s, ql_r, kz_s, kz_r, kx_s, kx_r, kf_s, kf_r, kc_s, kc_r, qy_s, qy_r, o_s, o_r, ho_s, ho_r,
):
    s = lax.axis_index("sp")
    t = lax.axis_index("tp")
    z = s // (Y * C)
    y = lax.rem(s // C, Y)
    c = lax.rem(s, C)
    gz = Z * 32
    groups = C * X

    def at(zz, yy, cc):
        return (zz * Y + yy) * C + cc

    def zpeer(k):
        return at(lax.rem(z + k, Z), y, c), t

    def ypeer(k):
        yy = lax.rem(y + k, Y)
        return yy, (at(z, yy, c), t)

    def xof(k):
        return lax.rem(t + k + X, X)

    def xpeer(k):
        return s, xof(k)

    other = (at(z, y, 1 - c), t)

    def remote(src, dst, ss, rs, who):
        return pltpu.make_async_remote_copy(
            src_ref=src, dst_ref=dst, send_sem=ss, recv_sem=rs, device_id=who, device_id_type=MESH
        )

    barrier = pltpu.get_barrier_semaphore()
    peers = [zpeer(k) for k in range(1, Z)] + [ypeer(k)[1] for k in range(1, Y)]
    peers += [xpeer(k) for k in range(1, X)] + [other]
    for who in peers:
        pl.semaphore_signal(barrier, inc=1, device_id=who, device_id_type=MESH)

    pairs = [
        (tok_h, tok), (qdown_h, qdown), (qlgain_h, qlgain), (ldown_h, ldown), (lgain_h, lgain), (rdown_h, rdown),
        (qup_h, qup), (qcols_h, qcols), (qgain_h, qgain), (kgain_h, kgain), (gcols_h, gcols), (vup_h, vup),
        (fine_h, fine), (coarse_h, coarse), (qsum_h, qsum), (kup_h, kup), (spread_h, spread), (ksum_h, ksum),
        (ogain_h, ogain), (oweight_h, oweight),
    ]
    loads = [pltpu.make_async_copy(a, b, in_s.at[i]) for i, (a, b) in enumerate(pairs)]
    for load in loads:
        load.start()
    sends = []

    def post(copy):
        copy.start()
        sends.append(copy)

    for load in loads[0:3]:
        load.wait()
    x = tok[...]
    qd = dot(x, qdown[...])
    qd = qd * lax.rsqrt(jnp.mean(qd * qd, axis=-1, keepdims=True) + EPS) * qlgain[...]
    qlbuf[t] = qd.astype(BF16)
    for load in loads[3:6]:
        load.wait()
    kd = dot(x, ldown[...])
    kd = kd * lax.rsqrt(jnp.mean(kd * kd, axis=-1, keepdims=True) + EPS) * lgain[...]
    klbuf[t, 0] = kd.astype(BF16)
    rope = rdown[...]
    rk4 = dot_t(x, jnp.concatenate([rope, rope, rope, rope], axis=0)).astype(BF16).astype(F32)
    group = lanes(8) // 32
    rkbuf[t, 0] = jnp.where(
        group == 0, rk4[0:8], jnp.where(group == 1, rk4[8:16], jnp.where(group == 2, rk4[16:24], rk4[24:32]))
    )

    pl.semaphore_wait(barrier, len(peers))

    for k in range(1, X):
        post(remote(qlbuf.at[t], qlbuf.at[t], ql_s.at[k], ql_r.at[k], xpeer(k)))
    order = offsets(Z)
    for i in range(1, Z):
        back = order.index((Z - order[i]) % Z)
        for n, buf in enumerate((klbuf, rkbuf)):
            post(remote(buf.at[t, 0], buf.at[t, back], kz_s.at[n, i], kz_r.at[n, back], zpeer(order[i])))

    def to_x(i):
        first, count = batches[i]
        for n, buf in enumerate((klbuf, rkbuf)):
            part = buf.at[t, pl.ds(first, count)]
            for d in range(2):
                post(remote(part, part, kx_s.at[n, d, i], kx_r.at[n, d, i], xpeer(1 - 2 * d)))

    to_x(0)

    for load in loads[6:]:
        load.wait()
    lane1 = lanes(1)
    starts = jnp.full((1, 128), 1 << 30, jnp.int32)
    ends = jnp.zeros((1, 128), jnp.int32)
    total = jnp.int32(0)
    for d in range(NDOC):
        starts = jnp.where(lane1 == DOC_LANE + d, total, starts)
        total = total + doclen[d]
        ends = jnp.where(lane1 == DOC_LANE + d, total, ends)
    bounds[0:1, :] = starts
    bounds[1:2, :] = ends
    for n, gain in enumerate((qgain, kgain)):
        high = gain[...].astype(BF16)
        rest = gain[...] - high.astype(F32)
        middle = rest.astype(BF16)
        low = (rest - middle.astype(F32)).astype(BF16)
        spots = sum(dot(jnp.broadcast_to(piece, (8, WIDTH)), gcols[...]) for piece in (high, middle, low))
        for i in range(3):
            gains[3 * n + i : 3 * n + i + 1, :] = spots[0:1, 128 * i : 128 * i + 128]
    qweight = dot(qcols[...], qup[...]).astype(BF16)
    vupt[...] = jnp.transpose(vup[...].astype(F32)).astype(BF16)

    def turn(block, first, count):
        cb = coarse[0, pl.ds(block, 1), :]
        sb = coarse[1, pl.ds(block, 1), :]
        cf = fine[0, pl.ds(first, count), :]
        sf = fine[1, pl.ds(first, count), :]
        return cb * cf - sb * sf, sb * cf + cb * sf

    for k in range(1, X):
        xx = xof(-k)
        remote(qlbuf.at[xx], qlbuf.at[xx], ql_s.at[k], ql_r.at[k], (s, xx)).wait_recv()
    ql = qlbuf[...].reshape(128, qlbuf.shape[2])
    qq = dot_t(ql, qweight)
    q0, q1, q2 = qq[:, 0:128], qq[:, 128:256], qq[:, 256:384]
    qs = head_sums(jnp.concatenate([q0 * q0, q1 * q1], axis=1), qsum[...])
    qs = lax.rsqrt(qs * (1.0 / WIDTH) + EPS)
    cosine, sine = turn(s, 0, 128)
    plain = q0 * qs[:, 0:128] * gains[0:1, :]
    rope = (q1 * gains[1:2, :] * cosine + q2 * gains[2:3, :] * sine) * qs[:, 128:256]
    qbuf[y, 0:128, :] = plain.astype(BF16)
    qbuf[y, 128:192, :] = jnp.where(lanes(64) < 64, rope[0:64], rope[64:128]).astype(BF16)
    for k in offsets(Y)[1:]:
        post(remote(qbuf.at[y], qbuf.at[y], qy_s.at[k], qy_r.at[k], ypeer(k)[1]))

    for i in range(1, len(batches)):
        first, count = batches[i]
        for slot in range(first, first + count):
            for n, buf in enumerate((klbuf, rkbuf)):
                remote(buf.at[t, 0], buf.at[t, slot], kz_s.at[n, slot], kz_r.at[n, slot], zpeer(order[slot])).wait_recv()
        to_x(i)

    def expand(xx):
        kl = klbuf[xx].reshape(gz, klbuf.shape[3])
        index = c * X + xx
        vtall[index] = dot_t(vupt[...], kl).astype(BF16)
        raw = dot(kl, kup[...])
        spreaded = dot(rkbuf[xx].reshape(Z * 8, 128).astype(BF16), spread[...])

        def rows_from(shift):
            return jnp.concatenate(
                [spreaded[8 * i : 8 * i + 8, 256 * g + shift : 256 * g + shift + 128] for i in range(Z) for g in range(4)],
                axis=0,
            )

        r1, r2 = rows_from(0), rows_from(128)
        sums = head_sums(jnp.concatenate([raw * raw, r1 * r1], axis=1), ksum[...])
        sums = lax.rsqrt(sums * (1.0 / WIDTH) + EPS)
        kall[index, :, 0:128] = (raw * sums[:, 0:128] * gains[3:4, :]).astype(BF16)
        first = pl.multiple_of(xx * 32, 32)
        for i in range(Z):
            block = at(lax.rem(z + order[i], Z), y, c)
            cosine, sine = turn(block, first, 32)
            part = slice(i * 32, i * 32 + 32)
            turned = (r1[part] * gains[4:5, :] * cosine + r2[part] * gains[5:6, :] * sine) * sums[part, 128:256]
            place = block * 128 + first + rows_of(32)
            inside = (place >= bounds[0:1, :]) & (place < bounds[1:2, :])
            kall[index, part, 128:256] = jnp.where(inside, 1.0, turned).astype(BF16)

    def to_core(xx):
        index = c * X + xx
        for n, buf in enumerate((kall, vtall)):
            post(remote(buf.at[index], buf.at[index], kc_s.at[n, xx], kc_r.at[n, xx], other))

    expand(t)
    for i, (first, count) in enumerate(batches):
        for d in range(2):
            xx = xof(2 * d - 1)
            for n, buf in enumerate((klbuf, rkbuf)):
                part = buf.at[xx, pl.ds(first, count)]
                remote(part, part, kx_s.at[n, d, i], kx_r.at[n, d, i], (s, xx)).wait_recv()
                if d == onward(i):
                    post(remote(part, part, kf_s.at[n, i], kf_r.at[n, i], xpeer(1 - 2 * d)))
    to_core(t)
    expand(xof(-1))
    expand(xof(1))
    for i, (first, count) in enumerate(batches):
        xx = xof(2)
        for n, buf in enumerate((klbuf, rkbuf)):
            part = buf.at[xx, pl.ds(first, count)]
            remote(part, part, kf_s.at[n, i], kf_r.at[n, i], xpeer(2 * onward(i) - 1)).wait_recv()
    to_core(xof(-1))
    to_core(xof(1))
    expand(xof(2))
    to_core(xof(2))
    for xx in range(X):
        index = (1 - c) * X + xx
        for n, buf in enumerate((kall, vtall)):
            remote(buf.at[index], buf.at[index], kc_s.at[n, xx], kc_r.at[n, xx], other).wait_recv()

    def attend(yy):
        block = at(z, yy, c)
        qplain = qbuf[yy, 0:128, :].astype(F32)
        qrope = qbuf[yy, 128:192, :].astype(F32)
        qrope = jnp.concatenate([qrope, pltpu.roll(qrope, 64, 1)], axis=0)
        place = block * 128 + rows_of(128)
        inside = (place >= bounds[0:1, :]) & (place < bounds[1:2, :])
        lane = lanes(128)
        apart = jnp.where((lane >= DOC_LANE) & (lane < DOC_LANE + NDOC) & jnp.logical_not(inside), APART, 0.0)
        both = []
        for h in range(2):
            left = jnp.where(lane // 64 == h, qplain, 0.0)
            right = jnp.where(lane // 32 == h, qrope, apart)
            both.append(jnp.concatenate([left, right], axis=1))
        queries = jnp.concatenate(both, axis=0).astype(BF16)
        scores = dot_t(kall[...].reshape(groups * gz, 256), queries)
        sbuf[...] = scores.reshape(groups, gz, 256)
        top = jnp.max(scores, axis=0, keepdims=True)
        count = None
        acc = None
        for g in range(groups):
            weights = jnp.exp2((sbuf[g] - top) * (SCALE * LOG2E))
            added = jnp.sum(weights, axis=0, keepdims=True)
            count = added if count is None else count + added
            update = dot(vtall[g], weights.astype(BF16))
            acc = update if acc is None else acc + update
        log = top * SCALE + jnp.log(count)
        lsend[yy] = jnp.where(rows_of(8) == 0, log[:, 0:128], log[:, 128:256])
        inv = 1.0 / count
        osend[yy, 0:64, :] = (acc[0:64, 0:128] * inv[:, 0:128]).astype(BF16)
        osend[yy, 64:128, :] = (acc[64:128, 128:256] * inv[:, 128:256]).astype(BF16)

    def step(i, carry):
        k = lax.rem(jnp.where(lax.rem(i, 2) == 1, (i + 1) // 2, Y - i // 2), Y)
        yy, who = ypeer(k)
        back = lax.rem(Y - k, Y)

        @pl.when(i > 0)
        def _():
            remote(qbuf.at[yy], qbuf.at[yy], qy_s.at[back], qy_r.at[back], who).wait_recv()

        attend(yy)

        @pl.when(i > 0)
        def _():
            remote(osend.at[yy], orecv.at[y], o_s.at[0, k], o_r.at[0, k], who).start()
            remote(lsend.at[yy], lrecv.at[y], o_s.at[1, k], o_r.at[1, k], who).start()

        return carry

    lax.fori_loop(0, Y, step, 0)

    orecv[y] = osend[y]
    lrecv[y] = lsend[y]
    for k in range(1, Y):
        yy, who = ypeer(Y - k)
        remote(osend.at[yy], orecv.at[yy], o_s.at[0, k], o_r.at[0, k], who).wait_recv()
        remote(lsend.at[yy], lrecv.at[yy], o_s.at[1, k], o_r.at[1, k], who).wait_recv()
    top = lrecv[0]
    for i in range(1, Y):
        top = jnp.maximum(top, lrecv[i])
    whole = jnp.zeros_like(top)
    acc0 = jnp.zeros((64, 128), F32)
    acc1 = jnp.zeros((64, 128), F32)
    for i in range(Y):
        weight = jnp.exp(lrecv[i] - top)
        whole = whole + weight
        acc0 = acc0 + weight[0:1] * orecv[i, 0:64, :].astype(F32)
        acc1 = acc1 + weight[1:2] * orecv[i, 64:128, :].astype(F32)
    logs[...] = (top + jnp.log(whole))[0:2]
    inv = 1.0 / whole
    heads = jnp.concatenate([acc0 * inv[0:1], acc1 * inv[1:2]], axis=0)
    hobuf[t] = jnp.transpose(heads).astype(BF16)
    for k in range(1, X):
        post(remote(hobuf.at[t], hobuf.at[t], ho_s.at[k], ho_r.at[k], xpeer(k)))
    for k in range(1, Y):
        yy, who = ypeer(k)
        remote(osend.at[yy], orecv.at[y], o_s.at[0, k], o_r.at[0, k], who).wait_send()
        remote(lsend.at[yy], lrecv.at[y], o_s.at[1, k], o_r.at[1, k], who).wait_send()
    for k in range(1, X):
        xx = xof(-k)
        remote(hobuf.at[xx], hobuf.at[xx], ho_s.at[k], ho_r.at[k], (s, xx)).wait_recv()
    full = jnp.concatenate([hobuf[i].astype(F32) for i in range(X)], axis=1)
    normed = full * lax.rsqrt(jnp.mean(full * full, axis=-1, keepdims=True) + EPS) * ogain[...]
    out[...] = dot(normed.astype(BF16), oweight[...]).astype(BF16)
    for copy in sends:
        copy.wait_send()


def onward(batch):
    return 0 if batch in (0, 3) else 1


def per_device(
    split, X,
    tokens, doc_lengths, query_down, latent_down, rope_down, query_latent_gain, latent_gain,
    query_up, key_up, value_up, query_gain, key_gain, output_gain, output_weight,
):
    Z, Y, C = split
    fine, coarse = tables(Z * Y * C)
    hbm = pl.BlockSpec(memory_space=pltpu.HBM)
    vm = pl.BlockSpec(memory_space=pltpu.VMEM)
    sm = pl.BlockSpec(memory_space=pltpu.SMEM)
    dma = pltpu.SemaphoreType.DMA
    gz = Z * 32
    groups = C * X
    batches = [(0, 1), (1, 2), (3, 2), (5, 3)] if Z == 8 else [(0, 1), (1, 1)]
    QR, KVR = query_down.shape[1], latent_down.shape[1]
    const = lambda a: jnp.asarray(a, BF16)
    row = lambda a: a.reshape(1, -1)
    inputs = [
        tokens, query_down, latent_down, rope_down.T, row(query_latent_gain), row(latent_gain),
        query_up.T, key_up, value_up, row(query_gain), row(key_gain), row(output_gain), output_weight,
        jnp.asarray(fine), jnp.asarray(coarse), const(query_columns().T), const(rope_spread()),
        const(sum_matrix(32)), const(sum_matrix(64)), const(gain_columns()),
    ]
    return pl.pallas_call(
        functools.partial(kernel, Z, Y, C, X, batches),
        out_shape=(
            jax.ShapeDtypeStruct((128, output_weight.shape[1]), BF16),
            jax.ShapeDtypeStruct((2, 128), F32),
        ),
        in_specs=[hbm, sm] + [hbm] * (len(inputs) - 1),
        out_specs=(vm, vm),
        scratch_shapes=[pltpu.VMEM(a.shape, a.dtype) for a in inputs] + [
            pltpu.VMEM((X, 32, QR), BF16),
            pltpu.VMEM((X, Z, 32, KVR), BF16),
            pltpu.VMEM((X, Z, 8, 128), F32),
            pltpu.VMEM((Y, 192, 128), BF16),
            pltpu.VMEM((groups, gz, 256), BF16),
            pltpu.VMEM((groups, 128, gz), BF16),
            pltpu.VMEM((groups, gz, 256), F32),
            pltpu.VMEM((128, KVR), BF16),
            pltpu.VMEM((Y, 128, 128), BF16),
            pltpu.VMEM((Y, 8, 128), F32),
            pltpu.VMEM((Y, 128, 128), BF16),
            pltpu.VMEM((Y, 8, 128), F32),
            pltpu.VMEM((X, 128, 128), BF16),
            pltpu.VMEM((8, 128), jnp.int32),
            pltpu.VMEM((8, 128), F32),
            dma((len(inputs),)),
            dma((X,)), dma((X,)),
            dma((2, Z)), dma((2, Z)),
            dma((2, 2, 4)), dma((2, 2, 4)),
            dma((2, 4)), dma((2, 4)),
            dma((2, X)), dma((2, X)),
            dma((Y,)), dma((Y,)),
            dma((2, Y)), dma((2, Y)),
            dma((X,)), dma((X,)),
        ],
        compiler_params=pltpu.CompilerParams(
            collective_id=0, has_side_effects=True, vmem_limit_bytes=60 * 2**20
        ),
    )(tokens, doc_lengths, *inputs[1:])


def solution(mesh):
    split = split_of(mesh.shape["sp"])
    return jax.shard_map(
        functools.partial(per_device, split, mesh.shape["tp"]),
        mesh=mesh,
        in_specs=(
            P(("sp", "tp"), None),
            P(), P(), P(), P(), P(), P(),
            P(None, "tp"), P(None, "tp"), P(None, "tp"),
            P(), P(), P(),
            P(None, "tp"),
        ),
        out_specs=(P("sp", "tp"), P("tp", "sp")),
        check_vma=False,
    )
```

```python
import functools

import jax
import jax.numpy as jnp
import numpy as np
from jax import lax
from jax.experimental import pallas as pl
from jax.experimental.pallas import tpu as pltpu
from jax.sharding import PartitionSpec as P

NOPE = 64
ROPE = 32
VD = 64
NDOC = 16
WIDTH = NOPE + ROPE
EPS = 1e-06
THETA = 10000.0
APART = -float(2**20)
SCALE = WIDTH**-0.5
LOG2E = 1.4426950408889634
F32 = jnp.float32
BF16 = jnp.bfloat16
MESH = pl.DeviceIdType.MESH
DOC_LANE = 64


def split_of(count):
    return {128: (8, 8, 2), 8: (2, 2, 2), 16: (2, 4, 2)}[count]


def tables(blocks):
    half = ROPE // 2
    inverse = THETA ** (-(np.arange(128) % half).astype(np.float64) / half)
    fine = np.arange(128)[:, None] * inverse[None]
    coarse = (np.arange(blocks) * 128)[:, None] * inverse[None]
    fine = np.stack([np.cos(fine), np.sin(fine)]).astype(np.float32)
    coarse = np.stack([np.cos(coarse), np.sin(coarse)]).astype(np.float32)
    return fine, coarse


def query_rows():
    out = np.zeros((256, 2 * WIDTH), np.float32)
    for j in range(128):
        out[j, (j // 64) * WIDTH + j % 64] = 1
    for j in range(64):
        head, entry = j // 32, j % 32
        out[128 + j, head * WIDTH + NOPE + entry] = 1
        out[192 + j, head * WIDTH + NOPE + (entry + 16) % 32] = 1
    return out


def rope_spread():
    out = np.zeros((128, 1024), np.float32)
    for g in range(4):
        for j in range(64):
            out[32 * g + j % 32, 256 * g + j] = 1
            out[32 * g + (j % 32 + 16) % 32, 256 * g + 128 + j] = 1
    return out


def sum_matrix():
    out = np.zeros((256, 256), np.float32)
    for col in range(256):
        head = col // 64 if col < 128 else ((col - 128) // 32) % 2
        for i in range(128):
            out[i, col] = i // 64 == head
        out[128:160, col] = 1
    return out


def dot(a, b):
    return jnp.dot(a, b, preferred_element_type=F32)


def dot_t(a, b):
    return lax.dot_general(a, b, (((1,), (1,)), ((), ())), preferred_element_type=F32)


def lanes(rows, width=128):
    return lax.broadcasted_iota(jnp.int32, (rows, width), 1)


def rows_of(rows, width=128):
    return lax.broadcasted_iota(jnp.int32, (rows, width), 0)


def head_sums(squares, matrix):
    high = squares.astype(BF16)
    low = (squares - high.astype(F32)).astype(BF16)
    return dot(high, matrix) + dot(low, matrix)


def offsets(count):
    return [(i + 1) // 2 if i % 2 else (count - i // 2) % count for i in range(count)]


def gain_columns():
    out = np.zeros((WIDTH, 384), np.float32)
    for j in range(128):
        entry = j % 32
        out[j % 64, j] = 1
        out[NOPE + entry, 128 + j] = 1
        out[NOPE + (entry + 16) % 32, 256 + j] = -1 if entry < 16 else 1
    return out


def kernel(
    Z, Y, C, X, batches,
    tok_h, doclen, qdown_h, ldown_h, rdown_h, qlgain_h, lgain_h, qup_h, kup_h, vup_h, qgain_h, kgain_h, ogain_h, oweight_h,
    fine_h, coarse_h, qcols_h, spread_h, ksum_h, gcols_h,
    out, logs,
    tok, qdown, ldown, rdown, qlgain, lgain, qup, kup, vup, qgain, kgain, ogain, oweight,
    fine, coarse, qcols, spread, ksum, gcols,
    qlbuf, klbuf, rkbuf, qbuf, kall, vtall, sbuf0, sbuf1, pbuf0, pbuf1, stats, qside, qtable, vupt, osend, lsend, orecv, lrecv, hobuf, bounds, columns, gains,
    in_s, ql_s, ql_r, kz_s, kz_r, kx_s, kx_r, kf_s, kf_r, kc_s, kc_r, qy_s, qy_r, o_s, o_r, ho_s, ho_r,
):
    s = lax.axis_index("sp")
    t = lax.axis_index("tp")
    z = s // (Y * C)
    y = lax.rem(s // C, Y)
    c = lax.rem(s, C)
    gz = Z * 32
    groups = C * X

    def at(zz, yy, cc):
        return (zz * Y + yy) * C + cc

    def zpeer(k):
        return at(lax.rem(z + k, Z), y, c), t

    def ypeer(k):
        yy = lax.rem(y + k, Y)
        return yy, (at(z, yy, c), t)

    def xof(k):
        return lax.rem(t + k + X, X)

    def xpeer(k):
        return s, xof(k)

    other = (at(z, y, 1 - c), t)

    def remote(src, dst, ss, rs, who):
        return pltpu.make_async_remote_copy(
            src_ref=src, dst_ref=dst, send_sem=ss, recv_sem=rs, device_id=who, device_id_type=MESH
        )

    pairs = [
        (tok_h, tok), (ldown_h, ldown), (lgain_h, lgain), (rdown_h, rdown), (qdown_h, qdown), (qlgain_h, qlgain),
        (qup_h, qup), (qcols_h, qcols), (qgain_h, qgain), (kgain_h, kgain), (gcols_h, gcols), (vup_h, vup),
        (fine_h, fine), (coarse_h, coarse), (kup_h, kup), (spread_h, spread), (ksum_h, ksum),
        (ogain_h, ogain), (oweight_h, oweight),
    ]
    loads = [pltpu.make_async_copy(a, b, in_s.at[i]) for i, (a, b) in enumerate(pairs)]
    for load in loads:
        load.start()
    barrier = pltpu.get_barrier_semaphore()
    peers = [zpeer(k) for k in range(1, Z)] + [ypeer(k)[1] for k in range(1, Y)]
    peers += [xpeer(k) for k in range(1, X)] + [other]
    for who in peers:
        pl.semaphore_signal(barrier, inc=1, device_id=who, device_id_type=MESH)

    sends = []

    def post(copy):
        copy.start()
        sends.append(copy)

    for load in loads[0:4]:
        load.wait()
    x = tok[...]
    kd = dot(x, ldown[...])
    kd = kd * lax.rsqrt(jnp.mean(kd * kd, axis=-1, keepdims=True) + EPS) * lgain[...]
    klbuf[t, 0] = kd.astype(BF16)
    rope = rdown[...]
    rk4 = dot_t(x, jnp.concatenate([rope, rope, rope, rope], axis=0)).astype(BF16).astype(F32)
    group = lanes(8) // 32
    rkbuf[t, 0] = jnp.where(
        group == 0, rk4[0:8], jnp.where(group == 1, rk4[8:16], jnp.where(group == 2, rk4[16:24], rk4[24:32]))
    )

    pl.semaphore_wait(barrier, len(peers))

    order = offsets(Z)
    for i in range(1, Z):
        back = order.index((Z - order[i]) % Z)
        for n, buf in enumerate((klbuf, rkbuf)):
            post(remote(buf.at[t, 0], buf.at[t, back], kz_s.at[n, i], kz_r.at[n, back], zpeer(order[i])))

    def to_x(i):
        first, count = batches[i]
        for n, buf in enumerate((klbuf, rkbuf)):
            part = buf.at[t, pl.ds(first, count)]
            for d in range(2):
                post(remote(part, part, kx_s.at[n, d, i], kx_r.at[n, d, i], xpeer(1 - 2 * d)))

    to_x(0)

    for load in loads[4:6]:
        load.wait()
    qd = dot(tok[...], qdown[...])
    qd = qd * lax.rsqrt(jnp.mean(qd * qd, axis=-1, keepdims=True) + EPS) * qlgain[...]
    qlbuf[t] = qd.astype(BF16)
    for k in range(1, X):
        post(remote(qlbuf.at[t], qlbuf.at[t], ql_s.at[k], ql_r.at[k], xpeer(k)))

    def from_z(i):
        first, count = batches[i]
        for slot in range(first, first + count):
            for n, buf in enumerate((klbuf, rkbuf)):
                remote(buf.at[t, 0], buf.at[t, slot], kz_s.at[n, slot], kz_r.at[n, slot], zpeer(order[slot])).wait_recv()
        to_x(i)

    for load in loads[6:]:
        load.wait()
    lane1 = lanes(1)
    starts = jnp.full((1, 128), 1 << 30, jnp.int32)
    ends = jnp.zeros((1, 128), jnp.int32)
    total = jnp.int32(0)
    for d in range(NDOC):
        starts = jnp.where(lane1 == DOC_LANE + d, total, starts)
        total = total + doclen[d]
        ends = jnp.where(lane1 == DOC_LANE + d, total, ends)
    bounds[0:1, :] = starts
    bounds[1:2, :] = ends
    which = rows_of(NDOC)
    total = jnp.int32(0)
    starts = jnp.zeros((NDOC, 128), jnp.int32)
    ends = jnp.zeros((NDOC, 128), jnp.int32)
    for d in range(NDOC):
        starts = jnp.where(which == d, total, starts)
        total = total + doclen[d]
        ends = jnp.where(which == d, total, ends)
    columns[0] = starts
    columns[1] = ends
    for n, gain in enumerate((qgain, kgain)):
        high = gain[...].astype(BF16)
        rest = gain[...] - high.astype(F32)
        middle = rest.astype(BF16)
        low = (rest - middle.astype(F32)).astype(BF16)
        spots = sum(dot(jnp.broadcast_to(piece, (8, WIDTH)), gcols[...]) for piece in (high, middle, low))
        for i in range(3):
            gains[3 * n + i : 3 * n + i + 1, :] = spots[0:1, 128 * i : 128 * i + 128]
    qweight = dot(qcols[...], qup[...]).astype(BF16)
    vupt[...] = jnp.transpose(vup[...].astype(F32)).astype(BF16)

    def turn(block, first, count):
        cb = coarse[0, pl.ds(block, 1), :]
        sb = coarse[1, pl.ds(block, 1), :]
        cf = fine[0, pl.ds(first, count), :]
        sf = fine[1, pl.ds(first, count), :]
        return cb * cf - sb * sf, sb * cf + cb * sf

    cosine, sine = turn(s, 0, 128)
    qtable[0:64, :] = jnp.transpose(cosine * gains[1:2, :])[0:64, :]
    qtable[64:128, :] = jnp.transpose(sine * gains[2:3, :])[0:64, :]
    qtable[128:256, :] = jnp.transpose(jnp.broadcast_to(gains[0:1, :], (128, 128)))
    qside[...] = jnp.zeros((256, 256), BF16)

    from_z(1)
    for k in range(1, X):
        xx = xof(-k)
        remote(qlbuf.at[xx], qlbuf.at[xx], ql_s.at[k], ql_r.at[k], (s, xx)).wait_recv()
    qq = dot_t(qweight, qlbuf[...].reshape(128, qlbuf.shape[2]))
    for h in range(2):
        q0 = qq[64 * h : 64 * h + 64]
        q1 = qq[128 + 32 * h : 160 + 32 * h]
        q2 = qq[192 + 32 * h : 224 + 32 * h]
        qs = jnp.sum(q0 * q0, axis=0, keepdims=True) + jnp.sum(q1 * q1, axis=0, keepdims=True)
        qs = lax.rsqrt(qs * (1.0 / WIDTH) + EPS)
        qbuf[y, 64 * h : 64 * h + 64, :] = (q0 * qs * qtable[128 + 64 * h : 192 + 64 * h, :]).astype(BF16)
        turned = q1 * qtable[32 * h : 32 * h + 32, :] + q2 * qtable[64 + 32 * h : 96 + 32 * h, :]
        qbuf[y, 128 + 32 * h : 160 + 32 * h, :] = (turned * qs).astype(BF16)
    for k in offsets(Y)[:0:-1]:
        post(remote(qbuf.at[y], qbuf.at[y], qy_s.at[k], qy_r.at[k], ypeer(k)[1]))

    for i in range(2, len(batches)):
        from_z(i)

    def expand(xx):
        kl = klbuf[xx].reshape(gz, klbuf.shape[3])
        index = c * X + xx
        vtall[index] = dot_t(vupt[...], kl).astype(BF16)
        raw = dot(kl, kup[...])
        spreaded = dot(rkbuf[xx].reshape(Z * 8, 128).astype(BF16), spread[...])

        def rows_from(shift):
            return jnp.concatenate(
                [spreaded[8 * i : 8 * i + 8, 256 * g + shift : 256 * g + shift + 128] for i in range(Z) for g in range(4)],
                axis=0,
            )

        r1, r2 = rows_from(0), rows_from(128)
        sums = head_sums(jnp.concatenate([raw * raw, r1 * r1], axis=1), ksum[...])
        sums = lax.rsqrt(sums * (1.0 / WIDTH) + EPS)
        kall[index, :, 0:128] = (raw * sums[:, 0:128] * gains[3:4, :]).astype(BF16)
        first = pl.multiple_of(xx * 32, 32)
        for i in range(Z):
            block = at(lax.rem(z + order[i], Z), y, c)
            cosine, sine = turn(block, first, 32)
            part = slice(i * 32, i * 32 + 32)
            turned = (r1[part] * gains[4:5, :] * cosine + r2[part] * gains[5:6, :] * sine) * sums[part, 128:256]
            place = block * 128 + first + rows_of(32)
            inside = (place >= bounds[0:1, :]) & (place < bounds[1:2, :])
            kall[index, part, 128:256] = jnp.where(inside, 1.0, turned).astype(BF16)

    def to_core(xx):
        index = c * X + xx
        for n, buf in enumerate((kall, vtall)):
            post(remote(buf.at[index], buf.at[index], kc_s.at[n, xx], kc_r.at[n, xx], other))

    expand(t)
    for i, (first, count) in enumerate(batches):
        for d in range(2):
            xx = xof(2 * d - 1)
            for n, buf in enumerate((klbuf, rkbuf)):
                part = buf.at[xx, pl.ds(first, count)]
                remote(part, part, kx_s.at[n, d, i], kx_r.at[n, d, i], (s, xx)).wait_recv()
                if d == onward(i):
                    post(remote(part, part, kf_s.at[n, i], kf_r.at[n, i], xpeer(1 - 2 * d)))
    to_core(t)
    expand(xof(-1))
    expand(xof(1))
    for i, (first, count) in enumerate(batches):
        xx = xof(2)
        for n, buf in enumerate((klbuf, rkbuf)):
            part = buf.at[xx, pl.ds(first, count)]
            remote(part, part, kf_s.at[n, i], kf_r.at[n, i], xpeer(2 * onward(i) - 1)).wait_recv()
    to_core(xof(-1))
    to_core(xof(1))
    expand(xof(2))
    to_core(xof(2))
    for xx in range(X):
        index = (1 - c) * X + xx
        for n, buf in enumerate((kall, vtall)):
            remote(buf.at[index], buf.at[index], kc_s.at[n, xx], kc_r.at[n, xx], other).wait_recv()

    sbufs, pbufs = (sbuf0, sbuf1), (pbuf0, pbuf1)

    def turn_of(i):
        j = Y - 1 - i
        return lax.rem(jnp.where(lax.rem(j, 2) == 1, (j + 1) // 2, Y - j // 2), Y)

    def prepare(i):
        yy, _ = ypeer(turn_of(i))
        place = at(z, yy, c) * 128 + lanes(NDOC)
        inside = (place >= columns[0]) & (place < columns[1])
        apart = jnp.where(inside, 0.0, APART).astype(BF16)
        for h in range(2):
            cols = slice(128 * h, 128 * h + 128)
            qside[64 * h : 64 * h + 64, cols] = qbuf[yy, 64 * h : 64 * h + 64, :]
            qside[128 + 32 * h : 160 + 32 * h, cols] = qbuf[yy, 128 + 32 * h : 160 + 32 * h, :]
            qside[128 + DOC_LANE : 128 + DOC_LANE + NDOC, cols] = apart
    def score(par, g, most):
        scores = dot(kall[g], qside[...])
        for r in range(gz // 8):
            part = scores[8 * r : 8 * r + 8]
            sbufs[par][g, 8 * r : 8 * r + 8, :] = part
            most[r % 2] = part if most[r % 2] is None else jnp.maximum(most[r % 2], part)

    def scored(par, most):
        top = jnp.max(jnp.maximum(most[0], most[1]), axis=0, keepdims=True)
        stats[par] = jnp.broadcast_to(top, (8, 256)) * (SCALE * LOG2E)

    def weigh(par, g, count):
        top = stats[par]
        for r in range(gz // 16):
            rows = slice(16 * r, 16 * r + 16)
            weights = [
                jnp.exp2(sbufs[par][g, 16 * r + o : 16 * r + o + 8, :] * (SCALE * LOG2E) - top) for o in (0, 8)
            ]
            pbufs[par][g, rows, :] = jnp.concatenate(weights, axis=0).astype(BF16)
            for o in range(2):
                count[o] = weights[o] if count[o] is None else count[o] + weights[o]

    def weighed(par, count):
        stats[2 + par] = jnp.broadcast_to(jnp.sum(count[0] + count[1], axis=0, keepdims=True), (8, 256))
        stats[4 + par] = stats[par] * (1.0 / LOG2E)

    def gather(par, g, accs):
        update = dot(vtall[g], pbufs[par][g])
        accs[g % 2] = update if accs[g % 2] is None else accs[g % 2] + update

    def gathered(i, par, accs):
        yy, _ = ypeer(turn_of(i))
        acc = accs[0] + accs[1]
        top, count = stats[4 + par, 0:1, :], stats[2 + par, 0:1, :]
        log = top + jnp.log(count)
        lsend[yy] = jnp.where(rows_of(8) == 0, log[:, 0:128], log[:, 128:256])
        inv = 1.0 / count
        osend[yy, 0:64, :] = (acc[0:64, 0:128] * inv[:, 0:128]).astype(BF16)
        osend[yy, 64:128, :] = (acc[64:128, 128:256] * inv[:, 128:256]).astype(BF16)

    def work(i, par, first, second, third):
        most, count, accs = [None, None], [None, None], [None, None]
        if first:
            prepare(i)
        for g in range(groups):
            if third:
                gather(par, g, accs)
            if first:
                score(par, g, most)
            if second:
                weigh(1 - par, g, count)
        if third:
            gathered(i - 2, par, accs)
        if first:
            scored(par, most)
        if second:
            weighed(1 - par, count)

    def receive(i):
        k = turn_of(i)
        yy, who = ypeer(k)
        back = lax.rem(Y - k, Y)
        remote(qbuf.at[yy], qbuf.at[yy], qy_s.at[back], qy_r.at[back], who).wait_recv()

    def give(i):
        k = turn_of(i)
        yy, who = ypeer(k)
        remote(osend.at[yy], orecv.at[y], o_s.at[0, k], o_r.at[0, k], who).start()
        remote(lsend.at[yy], lrecv.at[y], o_s.at[1, k], o_r.at[1, k], who).start()

    receive(jnp.int32(0))
    work(jnp.int32(0), 0, True, False, False)
    if Y > 2:
        receive(jnp.int32(1))
    work(jnp.int32(1), 1, True, True, False)

    def step(pair, carry):
        for par in range(2):
            i = 2 + 2 * pair + par

            @pl.when(i < Y - 1)
            def _():
                receive(i)

            work(i, par, True, True, True)
            give(i - 2)
        return carry

    lax.fori_loop(0, (Y - 2) // 2, step, 0)
    work(jnp.int32(Y), 0, False, True, True)
    give(jnp.int32(Y - 2))
    work(jnp.int32(Y + 1), 1, False, False, True)

    orecv[y] = osend[y]
    lrecv[y] = lsend[y]
    for k in range(1, Y):
        yy, who = ypeer(Y - k)
        remote(osend.at[yy], orecv.at[yy], o_s.at[0, k], o_r.at[0, k], who).wait_recv()
        remote(lsend.at[yy], lrecv.at[yy], o_s.at[1, k], o_r.at[1, k], who).wait_recv()
    top = lrecv[0]
    for i in range(1, Y):
        top = jnp.maximum(top, lrecv[i])
    whole = jnp.zeros_like(top)
    acc0 = jnp.zeros((64, 128), F32)
    acc1 = jnp.zeros((64, 128), F32)
    for i in range(Y):
        weight = jnp.exp(lrecv[i] - top)
        whole = whole + weight
        acc0 = acc0 + weight[0:1] * orecv[i, 0:64, :].astype(F32)
        acc1 = acc1 + weight[1:2] * orecv[i, 64:128, :].astype(F32)
    logs[...] = (top + jnp.log(whole))[0:2]
    inv = 1.0 / whole
    heads = jnp.concatenate([acc0 * inv[0:1], acc1 * inv[1:2]], axis=0)
    hobuf[t] = jnp.transpose(heads).astype(BF16)
    for k in range(1, X):
        post(remote(hobuf.at[t], hobuf.at[t], ho_s.at[k], ho_r.at[k], xpeer(k)))
    for k in range(1, Y):
        yy, who = ypeer(k)
        remote(osend.at[yy], orecv.at[y], o_s.at[0, k], o_r.at[0, k], who).wait_send()
        remote(lsend.at[yy], lrecv.at[y], o_s.at[1, k], o_r.at[1, k], who).wait_send()
    for k in range(1, X):
        xx = xof(-k)
        remote(hobuf.at[xx], hobuf.at[xx], ho_s.at[k], ho_r.at[k], (s, xx)).wait_recv()
    full = jnp.concatenate([hobuf[i].astype(F32) for i in range(X)], axis=1)
    normed = full * lax.rsqrt(jnp.mean(full * full, axis=-1, keepdims=True) + EPS) * ogain[...]
    out[...] = dot(normed.astype(BF16), oweight[...]).astype(BF16)
    for copy in sends:
        copy.wait_send()


def onward(batch):
    return 0 if batch in (0, 3) else 1


def per_device(
    split, X,
    tokens, doc_lengths, query_down, latent_down, rope_down, query_latent_gain, latent_gain,
    query_up, key_up, value_up, query_gain, key_gain, output_gain, output_weight,
):
    Z, Y, C = split
    fine, coarse = tables(Z * Y * C)
    hbm = pl.BlockSpec(memory_space=pltpu.HBM)
    vm = pl.BlockSpec(memory_space=pltpu.VMEM)
    sm = pl.BlockSpec(memory_space=pltpu.SMEM)
    dma = pltpu.SemaphoreType.DMA
    gz = Z * 32
    groups = C * X
    batches = [(0, 1), (1, 2), (3, 2), (5, 3)] if Z == 8 else [(0, 1), (1, 1)]
    QR, KVR = query_down.shape[1], latent_down.shape[1]
    const = lambda a: jnp.asarray(a, BF16)
    row = lambda a: a.reshape(1, -1)
    inputs = [
        tokens, query_down, latent_down, rope_down.T, row(query_latent_gain), row(latent_gain),
        query_up.T, key_up, value_up, row(query_gain), row(key_gain), row(output_gain), output_weight,
        jnp.asarray(fine), jnp.asarray(coarse), const(query_rows()), const(rope_spread()),
        const(sum_matrix()), const(gain_columns()),
    ]
    return pl.pallas_call(
        functools.partial(kernel, Z, Y, C, X, batches),
        out_shape=(
            pltpu.VMEM((128, output_weight.shape[1]), BF16),
            pltpu.VMEM((2, 128), F32),
        ),
        in_specs=[hbm, sm] + [hbm] * (len(inputs) - 1),
        out_specs=(vm, vm),
        scratch_shapes=[pltpu.VMEM(a.shape, a.dtype) for a in inputs] + [
            pltpu.VMEM((X, 32, QR), BF16),
            pltpu.VMEM((X, Z, 32, KVR), BF16),
            pltpu.VMEM((X, Z, 8, 128), F32),
            pltpu.VMEM((Y, 192, 128), BF16),
            pltpu.VMEM((groups, gz, 256), BF16),
            pltpu.VMEM((groups, 128, gz), BF16),
            pltpu.VMEM((groups, gz, 256), F32),
            pltpu.VMEM((groups, gz, 256), F32),
            pltpu.VMEM((groups, gz, 256), BF16),
            pltpu.VMEM((groups, gz, 256), BF16),
            pltpu.VMEM((6, 8, 256), F32),
            pltpu.VMEM((256, 256), BF16),
            pltpu.VMEM((256, 128), F32),
            pltpu.VMEM((128, KVR), BF16),
            pltpu.VMEM((Y, 128, 128), BF16),
            pltpu.VMEM((Y, 8, 128), F32),
            pltpu.VMEM((Y, 128, 128), BF16),
            pltpu.VMEM((Y, 8, 128), F32),
            pltpu.VMEM((X, 128, 128), BF16),
            pltpu.VMEM((8, 128), jnp.int32),
            pltpu.VMEM((2, NDOC, 128), jnp.int32),
            pltpu.VMEM((8, 128), F32),
            dma((len(inputs),)),
            dma((X,)), dma((X,)),
            dma((2, Z)), dma((2, Z)),
            dma((2, 2, 4)), dma((2, 2, 4)),
            dma((2, 4)), dma((2, 4)),
            dma((2, X)), dma((2, X)),
            dma((Y,)), dma((Y,)),
            dma((2, Y)), dma((2, Y)),
            dma((X,)), dma((X,)),
        ],
        compiler_params=pltpu.CompilerParams(
            collective_id=0, has_side_effects=True, vmem_limit_bytes=56 * 2**20
        ),
    )(tokens, doc_lengths, *inputs[1:])


def solution(mesh):
    split = split_of(mesh.shape["sp"])
    return jax.shard_map(
        functools.partial(per_device, split, mesh.shape["tp"]),
        mesh=mesh,
        in_specs=(
            P(("sp", "tp"), None),
            P(), P(), P(), P(), P(), P(),
            P(None, "tp"), P(None, "tp"), P(None, "tp"),
            P(), P(), P(),
            P(None, "tp"),
        ),
        out_specs=(P("sp", "tp"), P("tp", "sp")),
        check_vma=False,
    )
```

```python
import functools

import jax
import jax.numpy as jnp
import numpy as np
from jax import lax
from jax.experimental import pallas as pl
from jax.experimental.pallas import tpu as pltpu
from jax.sharding import PartitionSpec as P

NOPE = 64
ROPE = 32
VD = 64
NDOC = 16
WIDTH = NOPE + ROPE
EPS = 1e-06
THETA = 10000.0
APART = -float(2**20)
SCALE = WIDTH**-0.5
LOG2E = 1.4426950408889634
F32 = jnp.float32
BF16 = jnp.bfloat16
MESH = pl.DeviceIdType.MESH
DOC_LANE = 64


def split_of(count):
    return {128: (8, 8, 2), 8: (2, 2, 2), 16: (2, 4, 2)}[count]


def tables(blocks):
    half = ROPE // 2
    inverse = THETA ** (-(np.arange(128) % half).astype(np.float64) / half)
    fine = np.arange(128)[:, None] * inverse[None]
    coarse = (np.arange(blocks) * 128)[:, None] * inverse[None]
    fine = np.stack([np.cos(fine), np.sin(fine)]).astype(np.float32)
    coarse = np.stack([np.cos(coarse), np.sin(coarse)]).astype(np.float32)
    return fine, coarse


def query_rows():
    out = np.zeros((256, 2 * WIDTH), np.float32)
    for j in range(128):
        out[j, (j // 64) * WIDTH + j % 64] = 1
    for j in range(64):
        head, entry = j // 32, j % 32
        out[128 + j, head * WIDTH + NOPE + entry] = 1
        out[192 + j, head * WIDTH + NOPE + (entry + 16) % 32] = 1
    return out


def rope_spread():
    out = np.zeros((128, 1024), np.float32)
    for g in range(4):
        for j in range(64):
            out[32 * g + j % 32, 256 * g + j] = 1
            out[32 * g + (j % 32 + 16) % 32, 256 * g + 128 + j] = 1
    return out


def sum_matrix():
    out = np.zeros((256, 256), np.float32)
    for col in range(256):
        head = col // 64 if col < 128 else ((col - 128) // 32) % 2
        for i in range(128):
            out[i, col] = i // 64 == head
        out[128:160, col] = 1
    return out


def dot(a, b):
    return jnp.dot(a, b, preferred_element_type=F32)


def dot_t(a, b):
    return lax.dot_general(a, b, (((1,), (1,)), ((), ())), preferred_element_type=F32)


def lanes(rows, width=128):
    return lax.broadcasted_iota(jnp.int32, (rows, width), 1)


def rows_of(rows, width=128):
    return lax.broadcasted_iota(jnp.int32, (rows, width), 0)


def head_sums(squares, matrix):
    high = squares.astype(BF16)
    low = (squares - high.astype(F32)).astype(BF16)
    return dot(high, matrix) + dot(low, matrix)


def tiles(Z, Y):
    if (Z, Y) == (8, 8):
        keys = [(i % 8, 2 * i % 8) for i in (0, 1, 7, 4, 3, 5, 2, 6)]
        queries = [(2, 0), (-1, 1), (1, -1), (1, 0), (-1, 0), (0, 1), (0, -1), (0, 0)]
        batches = [(0, 1), (1, 2), (3, 3), (6, 2)]
    else:
        keys = [(i, 0) for i in range(Z)]
        queries = [(0, i) for i in range(Y - 1, -1, -1)]
        batches = [(0, 1), (1, Z - 1)]
    return keys, queries, batches


def gain_columns():
    out = np.zeros((WIDTH, 384), np.float32)
    for j in range(128):
        entry = j % 32
        out[j % 64, j] = 1
        out[NOPE + entry, 128 + j] = 1
        out[NOPE + (entry + 16) % 32, 256 + j] = -1 if entry < 16 else 1
    return out


def kernel(
    Z, Y, C, X, keys, queries, batches,
    tok_h, doclen, qdown_h, ldown_h, rdown_h, qlgain_h, lgain_h, qup_h, kup_h, vup_h, qgain_h, kgain_h, ogain_h, oweight_h,
    fine_h, coarse_h, qcols_h, spread_h, ksum_h, gcols_h,
    out, logs,
    tok, qdown, ldown, rdown, qlgain, lgain, qup, kup, vup, qgain, kgain, ogain, oweight,
    fine, coarse, qcols, spread, ksum, gcols,
    qlbuf, klbuf, rkbuf, qbuf, kall, vtall, sbuf0, sbuf1, pbuf0, pbuf1, stats, qside, qtable, vupt, osend, lsend, orecv, lrecv, hobuf, bounds, columns, gains,
    in_s, ql_s, ql_r, kz_s, kz_r, kx_s, kx_r, kf_s, kf_r, kc_s, kc_r, qy_s, qy_r, o_s, o_r, ho_s, ho_r,
):
    s = lax.axis_index("sp")
    t = lax.axis_index("tp")
    z = s // (Y * C)
    y = lax.rem(s // C, Y)
    c = lax.rem(s, C)
    gz = len(keys) * 32
    groups = C * X
    blocks = len(queries)
    side = 1 - 2 * c

    def at(zz, yy, cc):
        return (zz * Y + yy) * C + cc

    def chip(dz, dy):
        return lax.rem(z + dz + 2 * Z, Z), lax.rem(y + dy + 2 * Y, Y)

    def kpeer(i, way):
        return at(*chip(way * keys[i][0], way * keys[i][1]), c), t

    def picked(i, which):
        if isinstance(i, int):
            return queries[i][which]
        out = jnp.int32(0)
        for n, step in enumerate(queries):
            out = jnp.where(i == n, step[which], out)
        return out

    def qblock(i, way):
        return at(*chip(way * side * picked(i, 0), way * side * picked(i, 1)), c)

    def qpeer(i, way):
        return qblock(i, way), t

    def xof(k):
        return lax.rem(t + k + X, X)

    def xpeer(k):
        return s, xof(k)

    other = (at(z, y, 1 - c), t)

    def remote(src, dst, ss, rs, who):
        return pltpu.make_async_remote_copy(
            src_ref=src, dst_ref=dst, send_sem=ss, recv_sem=rs, device_id=who, device_id_type=MESH
        )

    pairs = [
        (tok_h, tok), (ldown_h, ldown), (lgain_h, lgain), (rdown_h, rdown), (qdown_h, qdown), (qlgain_h, qlgain),
        (qup_h, qup), (qcols_h, qcols), (qgain_h, qgain), (kgain_h, kgain), (gcols_h, gcols), (vup_h, vup),
        (fine_h, fine), (coarse_h, coarse), (kup_h, kup), (spread_h, spread), (ksum_h, ksum),
        (ogain_h, ogain), (oweight_h, oweight),
    ]
    loads = [pltpu.make_async_copy(a, b, in_s.at[i]) for i, (a, b) in enumerate(pairs)]
    for load in loads:
        load.start()
    barrier = pltpu.get_barrier_semaphore()
    near = {(w * dz % Z, w * dy % Y) for dz, dy in queries[:-1] for w in (1, -1)}
    peers = [(at(*chip(dz, dy), c), t) for dz, dy in sorted(near | set(keys[1:]))]
    peers += [xpeer(k) for k in range(1, X)] + [other]
    for who in peers:
        pl.semaphore_signal(barrier, inc=1, device_id=who, device_id_type=MESH)

    sends = []

    def post(copy):
        copy.start()
        sends.append(copy)

    for load in loads[0:4]:
        load.wait()
    x = tok[...]
    kd = dot(x, ldown[...])
    kd = kd * lax.rsqrt(jnp.mean(kd * kd, axis=-1, keepdims=True) + EPS) * lgain[...]
    klbuf[t, 0] = kd.astype(BF16)
    rope = rdown[...]
    rk4 = dot_t(x, jnp.concatenate([rope, rope, rope, rope], axis=0)).astype(BF16).astype(F32)
    group = lanes(8) // 32
    rkbuf[t, 0] = jnp.where(
        group == 0, rk4[0:8], jnp.where(group == 1, rk4[8:16], jnp.where(group == 2, rk4[16:24], rk4[24:32]))
    ).astype(BF16)

    pl.semaphore_wait(barrier, len(peers))

    for i in range(len(keys) - 1, 0, -1):
        for n, buf in enumerate((klbuf, rkbuf)):
            post(remote(buf.at[t, 0], buf.at[t, i], kz_s.at[n, i], kz_r.at[n, i], kpeer(i, -1)))

    def to_x(i):
        first, count = batches[i]
        for n, buf in enumerate((klbuf, rkbuf)):
            part = buf.at[t, pl.ds(first, count)]
            for d in range(2):
                post(remote(part, part, kx_s.at[n, d, i], kx_r.at[n, d, i], xpeer(1 - 2 * d)))

    to_x(0)

    for load in loads[4:6]:
        load.wait()
    qd = dot(tok[...], qdown[...])
    qd = qd * lax.rsqrt(jnp.mean(qd * qd, axis=-1, keepdims=True) + EPS) * qlgain[...]
    qlbuf[t] = qd.astype(BF16)
    for k in range(1, X):
        post(remote(qlbuf.at[t], qlbuf.at[t], ql_s.at[k], ql_r.at[k], xpeer(k)))

    def from_z(i):
        first, count = batches[i]
        for slot in range(first, first + count):
            for n, buf in enumerate((klbuf, rkbuf)):
                remote(buf.at[t, 0], buf.at[t, slot], kz_s.at[n, slot], kz_r.at[n, slot], kpeer(slot, 1)).wait_recv()
        to_x(i)

    for load in loads[6:]:
        load.wait()
    lane1 = lanes(1)
    starts = jnp.full((1, 128), 1 << 30, jnp.int32)
    ends = jnp.zeros((1, 128), jnp.int32)
    total = jnp.int32(0)
    for d in range(NDOC):
        starts = jnp.where(lane1 == DOC_LANE + d, total, starts)
        total = total + doclen[d]
        ends = jnp.where(lane1 == DOC_LANE + d, total, ends)
    bounds[0:1, :] = starts
    bounds[1:2, :] = ends
    which = rows_of(NDOC)
    total = jnp.int32(0)
    starts = jnp.zeros((NDOC, 128), jnp.int32)
    ends = jnp.zeros((NDOC, 128), jnp.int32)
    for d in range(NDOC):
        starts = jnp.where(which == d, total, starts)
        total = total + doclen[d]
        ends = jnp.where(which == d, total, ends)
    columns[0] = starts
    columns[1] = ends
    for n, gain in enumerate((qgain, kgain)):
        high = gain[...].astype(BF16)
        rest = gain[...] - high.astype(F32)
        middle = rest.astype(BF16)
        low = (rest - middle.astype(F32)).astype(BF16)
        spots = sum(dot(jnp.broadcast_to(piece, (8, WIDTH)), gcols[...]) for piece in (high, middle, low))
        for i in range(3):
            gains[3 * n + i : 3 * n + i + 1, :] = spots[0:1, 128 * i : 128 * i + 128]
    qweight = dot(qcols[...], qup[...]).astype(BF16)
    vupt[...] = jnp.transpose(vup[...].astype(F32)).astype(BF16)

    def turn(block, first, count):
        cb = coarse[0, pl.ds(block, 1), :]
        sb = coarse[1, pl.ds(block, 1), :]
        cf = fine[0, pl.ds(first, count), :]
        sf = fine[1, pl.ds(first, count), :]
        return cb * cf - sb * sf, sb * cf + cb * sf

    cosine, sine = turn(s, 0, 128)
    qtable[0:64, :] = jnp.transpose(cosine * gains[1:2, :])[0:64, :]
    qtable[64:128, :] = jnp.transpose(sine * gains[2:3, :])[0:64, :]
    qtable[128:256, :] = jnp.transpose(jnp.broadcast_to(gains[0:1, :], (128, 128)))
    qside[...] = jnp.zeros((256, 256), BF16)

    from_z(1)
    for k in range(1, X):
        xx = xof(-k)
        remote(qlbuf.at[xx], qlbuf.at[xx], ql_s.at[k], ql_r.at[k], (s, xx)).wait_recv()
    qq = dot_t(qweight, qlbuf[...].reshape(128, qlbuf.shape[2]))
    for h in range(2):
        q0 = qq[64 * h : 64 * h + 64]
        q1 = qq[128 + 32 * h : 160 + 32 * h]
        q2 = qq[192 + 32 * h : 224 + 32 * h]
        qs = jnp.sum(q0 * q0, axis=0, keepdims=True) + jnp.sum(q1 * q1, axis=0, keepdims=True)
        qs = lax.rsqrt(qs * (1.0 / WIDTH) + EPS)
        qbuf[blocks - 1, 64 * h : 64 * h + 64, :] = (q0 * qs * qtable[128 + 64 * h : 192 + 64 * h, :]).astype(BF16)
        turned = q1 * qtable[32 * h : 32 * h + 32, :] + q2 * qtable[64 + 32 * h : 96 + 32 * h, :]
        qbuf[blocks - 1, 128 + 32 * h : 160 + 32 * h, :] = (turned * qs).astype(BF16)
    for i in range(blocks - 1):
        post(remote(qbuf.at[blocks - 1], qbuf.at[i], qy_s.at[i], qy_r.at[i], qpeer(i, -1)))

    for i in range(2, len(batches)):
        from_z(i)

    def expand(xx):
        kl = klbuf[xx].reshape(gz, klbuf.shape[3])
        index = c * X + xx
        vtall[index] = dot_t(vupt[...], kl).astype(BF16)
        raw = dot(kl, kup[...])
        spreaded = dot(rkbuf[xx].astype(F32).reshape(gz // 4, 128).astype(BF16), spread[...])

        def rows_from(shift):
            return jnp.concatenate(
                [spreaded[8 * i : 8 * i + 8, 256 * g + shift : 256 * g + shift + 128] for i in range(len(keys)) for g in range(4)],
                axis=0,
            )

        r1, r2 = rows_from(0), rows_from(128)
        sums = head_sums(jnp.concatenate([raw * raw, r1 * r1], axis=1), ksum[...])
        sums = lax.rsqrt(sums * (1.0 / WIDTH) + EPS)
        kall[index, :, 0:128] = (raw * sums[:, 0:128] * gains[3:4, :]).astype(BF16)
        first = pl.multiple_of(xx * 32, 32)
        for i in range(len(keys)):
            block = at(*chip(*keys[i]), c)
            cosine, sine = turn(block, first, 32)
            part = slice(i * 32, i * 32 + 32)
            turned = (r1[part] * gains[4:5, :] * cosine + r2[part] * gains[5:6, :] * sine) * sums[part, 128:256]
            place = block * 128 + first + rows_of(32)
            inside = (place >= bounds[0:1, :]) & (place < bounds[1:2, :])
            kall[index, part, 128:256] = jnp.where(inside, 1.0, turned).astype(BF16)

    def to_core(xx):
        index = c * X + xx
        for n, buf in enumerate((kall, vtall)):
            post(remote(buf.at[index], buf.at[index], kc_s.at[n, xx], kc_r.at[n, xx], other))

    expand(t)
    for i, (first, count) in enumerate(batches):
        for d in range(2):
            xx = xof(2 * d - 1)
            for n, buf in enumerate((klbuf, rkbuf)):
                part = buf.at[xx, pl.ds(first, count)]
                remote(part, part, kx_s.at[n, d, i], kx_r.at[n, d, i], (s, xx)).wait_recv()
                if d == onward(i):
                    post(remote(part, part, kf_s.at[n, i], kf_r.at[n, i], xpeer(1 - 2 * d)))
    to_core(t)
    expand(xof(-1))
    expand(xof(1))
    for i, (first, count) in enumerate(batches):
        xx = xof(2)
        for n, buf in enumerate((klbuf, rkbuf)):
            part = buf.at[xx, pl.ds(first, count)]
            remote(part, part, kf_s.at[n, i], kf_r.at[n, i], xpeer(2 * onward(i) - 1)).wait_recv()
    to_core(xof(-1))
    to_core(xof(1))
    expand(xof(2))
    to_core(xof(2))
    for xx in range(X):
        index = (1 - c) * X + xx
        for n, buf in enumerate((kall, vtall)):
            remote(buf.at[index], buf.at[index], kc_s.at[n, xx], kc_r.at[n, xx], other).wait_recv()

    sbufs, pbufs = (sbuf0, sbuf1), (pbuf0, pbuf1)

    def prepare(i):
        place = qblock(i, 1) * 128 + lanes(NDOC)
        inside = (place >= columns[0]) & (place < columns[1])
        apart = jnp.where(inside, 0.0, APART).astype(BF16)
        for h in range(2):
            cols = slice(128 * h, 128 * h + 128)
            qside[64 * h : 64 * h + 64, cols] = qbuf[i, 64 * h : 64 * h + 64, :]
            qside[128 + 32 * h : 160 + 32 * h, cols] = qbuf[i, 128 + 32 * h : 160 + 32 * h, :]
            qside[128 + DOC_LANE : 128 + DOC_LANE + NDOC, cols] = apart
    def score(par, g, most):
        scores = dot(kall[g], qside[...])
        for r in range(gz // 8):
            part = scores[8 * r : 8 * r + 8]
            sbufs[par][g, 8 * r : 8 * r + 8, :] = part
            most[r % 2] = part if most[r % 2] is None else jnp.maximum(most[r % 2], part)

    def scored(par, most):
        top = jnp.max(jnp.maximum(most[0], most[1]), axis=0, keepdims=True)
        stats[par] = jnp.broadcast_to(top, (8, 256)) * (SCALE * LOG2E)

    def weigh(par, g, count):
        top = stats[par]
        for r in range(gz // 16):
            rows = slice(16 * r, 16 * r + 16)
            weights = [
                jnp.exp2(sbufs[par][g, 16 * r + o : 16 * r + o + 8, :] * (SCALE * LOG2E) - top) for o in (0, 8)
            ]
            pbufs[par][g, rows, :] = jnp.concatenate(weights, axis=0).astype(BF16)
            for o in range(2):
                count[o] = weights[o] if count[o] is None else count[o] + weights[o]

    def weighed(par, count):
        stats[2 + par] = jnp.broadcast_to(jnp.sum(count[0] + count[1], axis=0, keepdims=True), (8, 256))
        stats[4 + par] = stats[par] * (1.0 / LOG2E)

    def gather(par, g, accs):
        update = dot(vtall[g], pbufs[par][g])
        accs[g % 2] = update if accs[g % 2] is None else accs[g % 2] + update

    def gathered(i, par, accs):
        acc = accs[0] + accs[1]
        top, count = stats[4 + par, 0:1, :], stats[2 + par, 0:1, :]
        log = top + jnp.log(count)
        lsend[i] = jnp.where(rows_of(2) == 0, log[:, 0:128], log[:, 128:256])
        inv = 1.0 / count
        osend[i, 0:64, :] = (acc[0:64, 0:128] * inv[:, 0:128]).astype(BF16)
        osend[i, 64:128, :] = (acc[64:128, 128:256] * inv[:, 128:256]).astype(BF16)

    def work(i, par, first, second, third):
        most, count, accs = [None, None], [None, None], [None, None]
        if first:
            prepare(i)
        for g in range(groups):
            if third:
                gather(par, g, accs)
            if first:
                score(par, g, most)
            if second:
                weigh(1 - par, g, count)
        if third:
            gathered(i - 2, par, accs)
        if first:
            scored(par, most)
        if second:
            weighed(1 - par, count)

    def receive(i):
        remote(qbuf.at[blocks - 1], qbuf.at[i], qy_s.at[i], qy_r.at[i], qpeer(i, 1)).wait_recv()

    def results(i, way):
        who = qpeer(i, way)
        return (
            remote(osend.at[i], orecv.at[i], o_s.at[0, i], o_r.at[0, i], who),
            remote(lsend.at[i], lrecv.at[i], o_s.at[1, i], o_r.at[1, i], who),
        )

    def give(i):
        for copy in results(i, 1):
            copy.start()

    receive(jnp.int32(0))
    work(jnp.int32(0), 0, True, False, False)
    if blocks > 2:
        receive(jnp.int32(1))
    work(jnp.int32(1), 1, True, True, False)

    def step(pair, carry):
        for par in range(2):
            i = 2 + 2 * pair + par

            @pl.when(i < blocks - 1)
            def _():
                receive(i)

            work(i, par, True, True, True)
            give(i - 2)
        return carry

    lax.fori_loop(0, (blocks - 2) // 2, step, 0)
    work(jnp.int32(blocks), 0, False, True, True)
    give(jnp.int32(blocks - 2))
    work(jnp.int32(blocks + 1), 1, False, False, True)

    own = blocks - 1
    orecv[own] = osend[own]
    lrecv[own] = lsend[own]
    for i in range(own):
        for copy in results(i, -1):
            copy.wait_recv()
    top = lrecv[0]
    for i in range(1, blocks):
        top = jnp.maximum(top, lrecv[i])
    whole = jnp.zeros_like(top)
    acc0 = jnp.zeros((64, 128), F32)
    acc1 = jnp.zeros((64, 128), F32)
    for i in range(blocks):
        weight = jnp.exp(lrecv[i] - top)
        whole = whole + weight
        acc0 = acc0 + weight[0:1] * orecv[i, 0:64, :].astype(F32)
        acc1 = acc1 + weight[1:2] * orecv[i, 64:128, :].astype(F32)
    logs[...] = top + jnp.log(whole)
    inv = 1.0 / whole
    heads = jnp.concatenate([acc0 * inv[0:1], acc1 * inv[1:2]], axis=0)
    hobuf[t] = jnp.transpose(heads).astype(BF16)
    for k in range(1, X):
        post(remote(hobuf.at[t], hobuf.at[t], ho_s.at[k], ho_r.at[k], xpeer(k)))
    for i in range(own):
        for copy in results(i, 1):
            copy.wait_send()
    for k in range(1, X):
        xx = xof(-k)
        remote(hobuf.at[xx], hobuf.at[xx], ho_s.at[k], ho_r.at[k], (s, xx)).wait_recv()
    full = jnp.concatenate([hobuf[i].astype(F32) for i in range(X)], axis=1)
    normed = full * lax.rsqrt(jnp.mean(full * full, axis=-1, keepdims=True) + EPS) * ogain[...]
    out[...] = dot(normed.astype(BF16), oweight[...]).astype(BF16)
    for copy in sends:
        copy.wait_send()


def onward(batch):
    return batch % 2


def per_device(
    split, X,
    tokens, doc_lengths, query_down, latent_down, rope_down, query_latent_gain, latent_gain,
    query_up, key_up, value_up, query_gain, key_gain, output_gain, output_weight,
):
    Z, Y, C = split
    fine, coarse = tables(Z * Y * C)
    hbm = pl.BlockSpec(memory_space=pltpu.HBM)
    vm = pl.BlockSpec(memory_space=pltpu.VMEM)
    sm = pl.BlockSpec(memory_space=pltpu.SMEM)
    dma = pltpu.SemaphoreType.DMA
    keys, queries, batches = tiles(Z, Y)
    gz = len(keys) * 32
    groups = C * X
    Y, Z = len(queries), len(keys)
    QR, KVR = query_down.shape[1], latent_down.shape[1]
    const = lambda a: jnp.asarray(a, BF16)
    row = lambda a: a.reshape(1, -1)
    inputs = [
        tokens, query_down, latent_down, rope_down.T, row(query_latent_gain), row(latent_gain),
        query_up.T, key_up, value_up, row(query_gain), row(key_gain), row(output_gain), output_weight,
        jnp.asarray(fine), jnp.asarray(coarse), const(query_rows()), const(rope_spread()),
        const(sum_matrix()), const(gain_columns()),
    ]
    return pl.pallas_call(
        functools.partial(kernel, *split, X, keys, queries, batches),
        out_shape=(
            pltpu.VMEM((128, output_weight.shape[1]), BF16),
            pltpu.VMEM((2, 128), F32),
        ),
        in_specs=[hbm, sm] + [hbm] * (len(inputs) - 1),
        out_specs=(vm, vm),
        scratch_shapes=[pltpu.VMEM(a.shape, a.dtype) for a in inputs] + [
            pltpu.VMEM((X, 32, QR), BF16),
            pltpu.VMEM((X, Z, 32, KVR), BF16),
            pltpu.VMEM((X, Z, 8, 128), BF16),
            pltpu.VMEM((Y, 192, 128), BF16),
            pltpu.VMEM((groups, gz, 256), BF16),
            pltpu.VMEM((groups, 128, gz), BF16),
            pltpu.VMEM((groups, gz, 256), F32),
            pltpu.VMEM((groups, gz, 256), F32),
            pltpu.VMEM((groups, gz, 256), BF16),
            pltpu.VMEM((groups, gz, 256), BF16),
            pltpu.VMEM((6, 8, 256), F32),
            pltpu.VMEM((256, 256), BF16),
            pltpu.VMEM((256, 128), F32),
            pltpu.VMEM((128, KVR), BF16),
            pltpu.VMEM((Y, 128, 128), BF16),
            pltpu.VMEM((Y, 2, 128), F32),
            pltpu.VMEM((Y, 128, 128), BF16),
            pltpu.VMEM((Y, 2, 128), F32),
            pltpu.VMEM((X, 128, 128), BF16),
            pltpu.VMEM((8, 128), jnp.int32),
            pltpu.VMEM((2, NDOC, 128), jnp.int32),
            pltpu.VMEM((8, 128), F32),
            dma((len(inputs),)),
            dma((X,)), dma((X,)),
            dma((2, Z)), dma((2, Z)),
            dma((2, 2, 4)), dma((2, 2, 4)),
            dma((2, 4)), dma((2, 4)),
            dma((2, X)), dma((2, X)),
            dma((Y,)), dma((Y,)),
            dma((2, Y)), dma((2, Y)),
            dma((X,)), dma((X,)),
        ],
        compiler_params=pltpu.CompilerParams(
            collective_id=0, has_side_effects=True, vmem_limit_bytes=56 * 2**20,
        ),
    )(tokens, doc_lengths, *inputs[1:])


def solution(mesh):
    split = split_of(mesh.shape["sp"])
    return jax.shard_map(
        functools.partial(per_device, split, mesh.shape["tp"]),
        mesh=mesh,
        in_specs=(
            P(("sp", "tp"), None),
            P(), P(), P(), P(), P(), P(),
            P(None, "tp"), P(None, "tp"), P(None, "tp"),
            P(), P(), P(),
            P(None, "tp"),
        ),
        out_specs=(P("sp", "tp"), P("tp", "sp")),
        check_vma=False,
    )
```

```python
import functools

import jax
import jax.numpy as jnp
import numpy as np
from jax import lax
from jax.experimental import pallas as pl
from jax.experimental.pallas import tpu as pltpu
from jax.sharding import PartitionSpec as P

NOPE = 64
ROPE = 32
VD = 64
NDOC = 16
WIDTH = NOPE + ROPE
EPS = 1e-06
THETA = 10000.0
APART = -float(2**20)
SCALE = WIDTH**-0.5
LOG2E = 1.4426950408889634
F32 = jnp.float32
BF16 = jnp.bfloat16
MESH = pl.DeviceIdType.MESH
DOC_LANE = 64


def split_of(count):
    return {128: (8, 8, 2), 8: (2, 2, 2), 16: (2, 4, 2)}[count]


def tables(blocks):
    half = ROPE // 2
    inverse = THETA ** (-(np.arange(128) % half).astype(np.float64) / half)
    fine = np.arange(128)[:, None] * inverse[None]
    coarse = (np.arange(blocks) * 128)[:, None] * inverse[None]
    fine = np.stack([np.cos(fine), np.sin(fine)]).astype(np.float32)
    coarse = np.stack([np.cos(coarse), np.sin(coarse)]).astype(np.float32)
    return fine, coarse


def query_rows():
    out = np.zeros((256, 2 * WIDTH), np.float32)
    for j in range(128):
        out[j, (j // 64) * WIDTH + j % 64] = 1
    for j in range(64):
        head, entry = j // 32, j % 32
        out[128 + j, head * WIDTH + NOPE + entry] = 1
        out[192 + j, head * WIDTH + NOPE + (entry + 16) % 32] = 1
    return out


def rope_spread():
    out = np.zeros((128, 1024), np.float32)
    for g in range(4):
        for j in range(64):
            out[32 * g + j % 32, 256 * g + j] = 1
            out[32 * g + (j % 32 + 16) % 32, 256 * g + 128 + j] = 1
    return out


def sum_matrix():
    out = np.zeros((256, 256), np.float32)
    for col in range(256):
        head = col // 64 if col < 128 else ((col - 128) // 32) % 2
        for i in range(128):
            out[i, col] = i // 64 == head
        out[128:160, col] = 1
    return out


def dot(a, b):
    return jnp.dot(a, b, preferred_element_type=F32)


def dot_t(a, b):
    return lax.dot_general(a, b, (((1,), (1,)), ((), ())), preferred_element_type=F32)


def lanes(rows, width=128):
    return lax.broadcasted_iota(jnp.int32, (rows, width), 1)


def rows_of(rows, width=128):
    return lax.broadcasted_iota(jnp.int32, (rows, width), 0)


def head_sums(squares, matrix):
    high = squares.astype(BF16)
    low = (squares - high.astype(F32)).astype(BF16)
    return dot(high, matrix) + dot(low, matrix)


def tiles(Z, Y):
    if (Z, Y) == (8, 8):
        keys = [(i, 0) for i in range(8)]
        queries = [(0, 4), (0, -3), (0, 3), (0, -2), (0, 2), (0, -1), (0, 1), (0, 0)]
        batches = [(0, 1), (1, 3), (4, 2), (6, 2)]
    else:
        keys = [(i, 0) for i in range(Z)]
        queries = [(0, i) for i in range(Y - 1, -1, -1)]
        batches = [(0, 1), (1, Z - 1)]
    return keys, queries, batches


def finish(out, logs, out_h, logs_h, sems):
    copies = [pltpu.make_async_copy(out, out_h, sems.at[0]), pltpu.make_async_copy(logs, logs_h, sems.at[1])]
    for copy in copies:
        copy.start()
    for copy in copies:
        copy.wait()


def gain_columns():
    out = np.zeros((WIDTH, 384), np.float32)
    for j in range(128):
        entry = j % 32
        out[j % 64, j] = 1
        out[NOPE + entry, 128 + j] = 1
        out[NOPE + (entry + 16) % 32, 256 + j] = -1 if entry < 16 else 1
    return out


def kernel(
    Z, Y, C, X, keys, queries, batches,
    tok_h, doclen, qdown_h, ldown_h, rdown_h, qlgain_h, lgain_h, qup_h, kup_h, vup_h, qgain_h, kgain_h, ogain_h, oweight_h,
    fine_h, coarse_h, qcols_h, spread_h, ksum_h, gcols_h,
    out, logs,
    tok, qdown, ldown, rdown, qlgain, lgain, qup, kup, vup, qgain, kgain, ogain, oweight,
    fine, coarse, qcols, spread, ksum, gcols,
    qlbuf, klbuf, rkbuf, qbuf, kall, vtall, sbuf0, sbuf1, pbuf0, pbuf1, stats, qside, qtable, vupt, osend, lsend, orecv, lrecv, hobuf, bounds, columns, gains,
    in_s, ql_s, ql_r, kz_s, kz_r, kx_s, kx_r, kf_s, kf_r, kc_s, kc_r, qy_s, qy_r, o_s, o_r, ho_s, ho_r,
):
    s = lax.axis_index("sp")
    t = lax.axis_index("tp")
    z = s // (Y * C)
    y = lax.rem(s // C, Y)
    c = lax.rem(s, C)
    gz = len(keys) * 32
    groups = C * X
    blocks = len(queries)
    side = 1 - 2 * c

    def at(zz, yy, cc):
        return (zz * Y + yy) * C + cc

    def chip(dz, dy):
        return lax.rem(z + dz + 2 * Z, Z), lax.rem(y + dy + 2 * Y, Y)

    def kpeer(i, way):
        return at(*chip(way * keys[i][0], way * keys[i][1]), c), t

    def picked(i, which):
        if isinstance(i, int):
            return queries[i][which]
        out = jnp.int32(0)
        for n, step in enumerate(queries):
            out = jnp.where(i == n, step[which], out)
        return out

    def qblock(i, way):
        return at(*chip(way * side * picked(i, 0), way * side * picked(i, 1)), c)

    def qpeer(i, way):
        return qblock(i, way), t

    def xof(k):
        return lax.rem(t + k + X, X)

    def xpeer(k):
        return s, xof(k)

    other = (at(z, y, 1 - c), t)

    def remote(src, dst, ss, rs, who):
        return pltpu.make_async_remote_copy(
            src_ref=src, dst_ref=dst, send_sem=ss, recv_sem=rs, device_id=who, device_id_type=MESH
        )

    pairs = [
        (tok_h, tok), (ldown_h, ldown), (lgain_h, lgain), (rdown_h, rdown), (qdown_h, qdown), (qlgain_h, qlgain),
        (qup_h, qup), (qcols_h, qcols), (qgain_h, qgain), (kgain_h, kgain), (gcols_h, gcols), (vup_h, vup),
        (fine_h, fine), (coarse_h, coarse), (kup_h, kup), (spread_h, spread), (ksum_h, ksum),
        (ogain_h, ogain), (oweight_h, oweight),
    ]
    loads = [pltpu.make_async_copy(a, b, in_s.at[i]) for i, (a, b) in enumerate(pairs)]
    for load in loads[:4]:
        load.start()
    barrier = pltpu.get_barrier_semaphore()
    near = {(w * dz % Z, w * dy % Y) for dz, dy in queries[:-1] for w in (1, -1)}
    peers = [(at(*chip(dz, dy), c), t) for dz, dy in sorted(near | set(keys[1:]))]
    peers += [xpeer(k) for k in range(1, X)] + [other]
    for who in peers:
        pl.semaphore_signal(barrier, inc=1, device_id=who, device_id_type=MESH)

    sends = []

    def post(copy):
        copy.start()
        sends.append(copy)

    for load in loads[0:4]:
        load.wait()
    for load in loads[4:]:
        load.start()
    x = tok[...]
    kd = dot(x, ldown[...])
    kd = kd * lax.rsqrt(jnp.mean(kd * kd, axis=-1, keepdims=True) + EPS) * lgain[...]
    klbuf[t, 0] = kd.astype(BF16)
    rope = rdown[...]
    rk4 = dot_t(x, jnp.concatenate([rope, rope, rope, rope], axis=0)).astype(BF16).astype(F32)
    group = lanes(8) // 32
    rkbuf[t, 0] = jnp.where(
        group == 0, rk4[0:8], jnp.where(group == 1, rk4[8:16], jnp.where(group == 2, rk4[16:24], rk4[24:32]))
    ).astype(BF16)

    pl.semaphore_wait(barrier, len(peers))

    for i in range(len(keys) - 1, 0, -1):
        for n, buf in enumerate((klbuf, rkbuf)):
            post(remote(buf.at[t, 0], buf.at[t, i], kz_s.at[n, i], kz_r.at[n, i], kpeer(i, -1)))

    def to_x(i):
        first, count = batches[i]
        for n, buf in enumerate((klbuf, rkbuf)):
            part = buf.at[t, pl.ds(first, count)]
            for d in range(2):
                post(remote(part, part, kx_s.at[n, d, i], kx_r.at[n, d, i], xpeer(1 - 2 * d)))

    to_x(0)

    for load in loads[4:6]:
        load.wait()
    qd = dot(tok[...], qdown[...])
    qd = qd * lax.rsqrt(jnp.mean(qd * qd, axis=-1, keepdims=True) + EPS) * qlgain[...]
    qlbuf[t] = qd.astype(BF16)
    for k in range(1, X):
        post(remote(qlbuf.at[t], qlbuf.at[t], ql_s.at[k], ql_r.at[k], xpeer(k)))

    def from_z(i):
        first, count = batches[i]
        for slot in range(first, first + count):
            for n, buf in enumerate((klbuf, rkbuf)):
                remote(buf.at[t, 0], buf.at[t, slot], kz_s.at[n, slot], kz_r.at[n, slot], kpeer(slot, 1)).wait_recv()
        to_x(i)

    for load in loads[6:]:
        load.wait()
    lane1 = lanes(1)
    starts = jnp.full((1, 128), 1 << 30, jnp.int32)
    ends = jnp.zeros((1, 128), jnp.int32)
    total = jnp.int32(0)
    for d in range(NDOC):
        starts = jnp.where(lane1 == DOC_LANE + d, total, starts)
        total = total + doclen[d]
        ends = jnp.where(lane1 == DOC_LANE + d, total, ends)
    bounds[0:1, :] = starts
    bounds[1:2, :] = ends
    which = rows_of(NDOC)
    total = jnp.int32(0)
    starts = jnp.zeros((NDOC, 128), jnp.int32)
    ends = jnp.zeros((NDOC, 128), jnp.int32)
    for d in range(NDOC):
        starts = jnp.where(which == d, total, starts)
        total = total + doclen[d]
        ends = jnp.where(which == d, total, ends)
    columns[0] = starts
    columns[1] = ends
    for n, gain in enumerate((qgain, kgain)):
        high = gain[...].astype(BF16)
        rest = gain[...] - high.astype(F32)
        middle = rest.astype(BF16)
        low = (rest - middle.astype(F32)).astype(BF16)
        spots = sum(dot(jnp.broadcast_to(piece, (8, WIDTH)), gcols[...]) for piece in (high, middle, low))
        for i in range(3):
            gains[3 * n + i : 3 * n + i + 1, :] = spots[0:1, 128 * i : 128 * i + 128]
    qweight = dot(qcols[...], qup[...]).astype(BF16)
    vupt[...] = jnp.transpose(vup[...].astype(F32)).astype(BF16)

    def turn(block, first, count):
        cb = coarse[0, pl.ds(block, 1), :]
        sb = coarse[1, pl.ds(block, 1), :]
        cf = fine[0, pl.ds(first, count), :]
        sf = fine[1, pl.ds(first, count), :]
        return cb * cf - sb * sf, sb * cf + cb * sf

    cosine, sine = turn(s, 0, 128)
    qtable[0:64, :] = jnp.transpose(cosine * gains[1:2, :])[0:64, :]
    qtable[64:128, :] = jnp.transpose(sine * gains[2:3, :])[0:64, :]
    qtable[128:256, :] = jnp.transpose(jnp.broadcast_to(gains[0:1, :], (128, 128)))
    qside[...] = jnp.zeros((256, 256), BF16)

    from_z(1)
    for k in range(1, X):
        xx = xof(-k)
        remote(qlbuf.at[xx], qlbuf.at[xx], ql_s.at[k], ql_r.at[k], (s, xx)).wait_recv()
    qq = dot_t(qweight, qlbuf[...].reshape(128, qlbuf.shape[2]))
    for h in range(2):
        q0 = qq[64 * h : 64 * h + 64]
        q1 = qq[128 + 32 * h : 160 + 32 * h]
        q2 = qq[192 + 32 * h : 224 + 32 * h]
        qs = jnp.sum(q0 * q0, axis=0, keepdims=True) + jnp.sum(q1 * q1, axis=0, keepdims=True)
        qs = lax.rsqrt(qs * (1.0 / WIDTH) + EPS)
        qbuf[blocks - 1, 64 * h : 64 * h + 64, :] = (q0 * qs * qtable[128 + 64 * h : 192 + 64 * h, :]).astype(BF16)
        turned = q1 * qtable[32 * h : 32 * h + 32, :] + q2 * qtable[64 + 32 * h : 96 + 32 * h, :]
        qbuf[blocks - 1, 128 + 32 * h : 160 + 32 * h, :] = (turned * qs).astype(BF16)
    for i in range(blocks - 1):
        post(remote(qbuf.at[blocks - 1], qbuf.at[i], qy_s.at[i], qy_r.at[i], qpeer(i, -1)))

    for i in range(2, len(batches)):
        from_z(i)

    def expand(xx):
        kl = klbuf[xx].reshape(gz, klbuf.shape[3])
        index = c * X + xx
        vtall[index] = dot_t(vupt[...], kl).astype(BF16)
        raw = dot(kl, kup[...])
        spreaded = dot(rkbuf[xx].astype(F32).reshape(gz // 4, 128).astype(BF16), spread[...])

        def rows_from(shift):
            return jnp.concatenate(
                [spreaded[8 * i : 8 * i + 8, 256 * g + shift : 256 * g + shift + 128] for i in range(len(keys)) for g in range(4)],
                axis=0,
            )

        r1, r2 = rows_from(0), rows_from(128)
        sums = head_sums(jnp.concatenate([raw * raw, r1 * r1], axis=1), ksum[...])
        sums = lax.rsqrt(sums * (1.0 / WIDTH) + EPS)
        kall[index, :, 0:128] = (raw * sums[:, 0:128] * gains[3:4, :]).astype(BF16)
        first = pl.multiple_of(xx * 32, 32)
        for i in range(len(keys)):
            block = at(*chip(*keys[i]), c)
            cosine, sine = turn(block, first, 32)
            part = slice(i * 32, i * 32 + 32)
            turned = (r1[part] * gains[4:5, :] * cosine + r2[part] * gains[5:6, :] * sine) * sums[part, 128:256]
            place = block * 128 + first + rows_of(32)
            inside = (place >= bounds[0:1, :]) & (place < bounds[1:2, :])
            kall[index, part, 128:256] = jnp.where(inside, 1.0, turned).astype(BF16)

    def to_core(xx):
        index = c * X + xx
        for n, buf in enumerate((kall, vtall)):
            post(remote(buf.at[index], buf.at[index], kc_s.at[n, xx], kc_r.at[n, xx], other))

    expand(t)
    for i, (first, count) in enumerate(batches):
        for d in range(2):
            xx = xof(2 * d - 1)
            for n, buf in enumerate((klbuf, rkbuf)):
                part = buf.at[xx, pl.ds(first, count)]
                remote(part, part, kx_s.at[n, d, i], kx_r.at[n, d, i], (s, xx)).wait_recv()
                if d == onward(i):
                    post(remote(part, part, kf_s.at[n, i], kf_r.at[n, i], xpeer(1 - 2 * d)))
    to_core(t)
    expand(xof(-1))
    expand(xof(1))
    for i, (first, count) in enumerate(batches):
        xx = xof(2)
        for n, buf in enumerate((klbuf, rkbuf)):
            part = buf.at[xx, pl.ds(first, count)]
            remote(part, part, kf_s.at[n, i], kf_r.at[n, i], xpeer(2 * onward(i) - 1)).wait_recv()
    to_core(xof(-1))
    to_core(xof(1))
    expand(xof(2))
    to_core(xof(2))
    for xx in range(X):
        index = (1 - c) * X + xx
        for n, buf in enumerate((kall, vtall)):
            remote(buf.at[index], buf.at[index], kc_s.at[n, xx], kc_r.at[n, xx], other).wait_recv()

    sbufs, pbufs = (sbuf0, sbuf1), (pbuf0, pbuf1)

    def prepare(i):
        place = qblock(i, 1) * 128 + lanes(NDOC)
        inside = (place >= columns[0]) & (place < columns[1])
        apart = jnp.where(inside, 0.0, APART).astype(BF16)
        for h in range(2):
            cols = slice(128 * h, 128 * h + 128)
            qside[64 * h : 64 * h + 64, cols] = qbuf[i, 64 * h : 64 * h + 64, :]
            qside[128 + 32 * h : 160 + 32 * h, cols] = qbuf[i, 128 + 32 * h : 160 + 32 * h, :]
            qside[128 + DOC_LANE : 128 + DOC_LANE + NDOC, cols] = apart
    def score(par, g, most):
        scores = dot(kall[g], qside[...])
        for r in range(gz // 8):
            part = scores[8 * r : 8 * r + 8]
            sbufs[par][g, 8 * r : 8 * r + 8, :] = part
            most[r % 2] = part if most[r % 2] is None else jnp.maximum(most[r % 2], part)

    def scored(par, most):
        top = jnp.max(jnp.maximum(most[0], most[1]), axis=0, keepdims=True)
        stats[par] = jnp.broadcast_to(top, (8, 256)) * (SCALE * LOG2E)

    def weigh(par, g, count):
        top = stats[par]
        for r in range(gz // 16):
            rows = slice(16 * r, 16 * r + 16)
            weights = [
                jnp.exp2(sbufs[par][g, 16 * r + o : 16 * r + o + 8, :] * (SCALE * LOG2E) - top) for o in (0, 8)
            ]
            pbufs[par][g, rows, :] = jnp.concatenate(weights, axis=0).astype(BF16)
            for o in range(2):
                count[o] = weights[o] if count[o] is None else count[o] + weights[o]

    def weighed(par, count):
        stats[2 + par] = jnp.broadcast_to(jnp.sum(count[0] + count[1], axis=0, keepdims=True), (8, 256))
        stats[4 + par] = stats[par] * (1.0 / LOG2E)

    def gather(par, g, accs):
        update = dot(vtall[g], pbufs[par][g])
        accs[g % 2] = update if accs[g % 2] is None else accs[g % 2] + update

    def gathered(i, par, accs):
        acc = accs[0] + accs[1]
        top, count = stats[4 + par, 0:1, :], stats[2 + par, 0:1, :]
        log = top + jnp.log(count)
        lsend[i] = jnp.where(rows_of(2) == 0, log[:, 0:128], log[:, 128:256])
        inv = 1.0 / count
        osend[i, 0:64, :] = (acc[0:64, 0:128] * inv[:, 0:128]).astype(BF16)
        osend[i, 64:128, :] = (acc[64:128, 128:256] * inv[:, 128:256]).astype(BF16)

    def work(i, par, first, second, third):
        most, count, accs = [None, None], [None, None], [None, None]
        if first:
            prepare(i)
        for g in range(groups):
            if third:
                gather(par, g, accs)
            if first:
                score(par, g, most)
            if second:
                weigh(1 - par, g, count)
        if third:
            gathered(i - 2, par, accs)
        if first:
            scored(par, most)
        if second:
            weighed(1 - par, count)

    def receive(i):
        remote(qbuf.at[blocks - 1], qbuf.at[i], qy_s.at[i], qy_r.at[i], qpeer(i, 1)).wait_recv()

    def results(i, way):
        who = qpeer(i, way)
        return (
            remote(osend.at[i], orecv.at[i], o_s.at[0, i], o_r.at[0, i], who),
            remote(lsend.at[i], lrecv.at[i], o_s.at[1, i], o_r.at[1, i], who),
        )

    def give(i):
        for copy in results(i, 1):
            copy.start()

    receive(jnp.int32(0))
    work(jnp.int32(0), 0, True, False, False)
    if blocks > 2:
        receive(jnp.int32(1))
    work(jnp.int32(1), 1, True, True, False)

    def step(pair, carry):
        for par in range(2):
            i = 2 + 2 * pair + par

            @pl.when(i < blocks - 1)
            def _():
                receive(i)

            work(i, par, True, True, True)
            give(i - 2)
        return carry

    lax.fori_loop(0, (blocks - 2) // 2, step, 0)
    work(jnp.int32(blocks), 0, False, True, True)
    give(jnp.int32(blocks - 2))
    work(jnp.int32(blocks + 1), 1, False, False, True)

    own = blocks - 1
    orecv[own] = osend[own]
    lrecv[own] = lsend[own]
    for i in range(own):
        for copy in results(i, -1):
            copy.wait_recv()
    top = lrecv[0]
    for i in range(1, blocks):
        top = jnp.maximum(top, lrecv[i])
    whole = jnp.zeros_like(top)
    acc0 = jnp.zeros((64, 128), F32)
    acc1 = jnp.zeros((64, 128), F32)
    for i in range(blocks):
        weight = jnp.exp(lrecv[i] - top)
        whole = whole + weight
        acc0 = acc0 + weight[0:1] * orecv[i, 0:64, :].astype(F32)
        acc1 = acc1 + weight[1:2] * orecv[i, 64:128, :].astype(F32)
    logs[...] = top + jnp.log(whole)
    inv = 1.0 / whole
    heads = jnp.concatenate([acc0 * inv[0:1], acc1 * inv[1:2]], axis=0)
    hobuf[t] = jnp.transpose(heads).astype(BF16)
    for k in range(1, X):
        post(remote(hobuf.at[t], hobuf.at[t], ho_s.at[k], ho_r.at[k], xpeer(k)))
    for i in range(own):
        for copy in results(i, 1):
            copy.wait_send()
    for k in range(1, X):
        xx = xof(-k)
        remote(hobuf.at[xx], hobuf.at[xx], ho_s.at[k], ho_r.at[k], (s, xx)).wait_recv()
    full = jnp.concatenate([hobuf[i].astype(F32) for i in range(X)], axis=1)
    normed = full * lax.rsqrt(jnp.mean(full * full, axis=-1, keepdims=True) + EPS) * ogain[...]
    out[...] = dot(normed.astype(BF16), oweight[...]).astype(BF16)
    for copy in sends:
        copy.wait_send()


def onward(batch):
    return (0, 1, 0, 1)[batch]


def per_device(
    split, X,
    tokens, doc_lengths, query_down, latent_down, rope_down, query_latent_gain, latent_gain,
    query_up, key_up, value_up, query_gain, key_gain, output_gain, output_weight,
):
    Z, Y, C = split
    fine, coarse = tables(Z * Y * C)
    hbm = pl.BlockSpec(memory_space=pltpu.HBM)
    vm = pl.BlockSpec(memory_space=pltpu.VMEM)
    sm = pl.BlockSpec(memory_space=pltpu.SMEM)
    dma = pltpu.SemaphoreType.DMA
    keys, queries, batches = tiles(Z, Y)
    gz = len(keys) * 32
    groups = C * X
    Y, Z = len(queries), len(keys)
    QR, KVR = query_down.shape[1], latent_down.shape[1]
    const = lambda a: jnp.asarray(a, BF16)
    row = lambda a: a.reshape(1, -1)
    inputs = [
        tokens, query_down, latent_down, rope_down.T, row(query_latent_gain), row(latent_gain),
        query_up.T, key_up, value_up, row(query_gain), row(key_gain), row(output_gain), output_weight,
        jnp.asarray(fine), jnp.asarray(coarse), const(query_rows()), const(rope_spread()),
        const(sum_matrix()), const(gain_columns()),
    ]
    results = pl.pallas_call(
        functools.partial(kernel, *split, X, keys, queries, batches),
        out_shape=(
            pltpu.VMEM((128, output_weight.shape[1]), BF16),
            pltpu.VMEM((2, 128), F32),
        ),
        in_specs=[hbm, sm] + [hbm] * (len(inputs) - 1),
        out_specs=(vm, vm),
        scratch_shapes=[pltpu.VMEM(a.shape, a.dtype) for a in inputs] + [
            pltpu.VMEM((X, 32, QR), BF16),
            pltpu.VMEM((X, Z, 32, KVR), BF16),
            pltpu.VMEM((X, Z, 8, 128), BF16),
            pltpu.VMEM((Y, 192, 128), BF16),
            pltpu.VMEM((groups, gz, 256), BF16),
            pltpu.VMEM((groups, 128, gz), BF16),
            pltpu.VMEM((groups, gz, 256), F32),
            pltpu.VMEM((groups, gz, 256), F32),
            pltpu.VMEM((groups, gz, 256), BF16),
            pltpu.VMEM((groups, gz, 256), BF16),
            pltpu.VMEM((6, 8, 256), F32),
            pltpu.VMEM((256, 256), BF16),
            pltpu.VMEM((256, 128), F32),
            pltpu.VMEM((128, KVR), BF16),
            pltpu.VMEM((Y, 128, 128), BF16),
            pltpu.VMEM((Y, 2, 128), F32),
            pltpu.VMEM((Y, 128, 128), BF16),
            pltpu.VMEM((Y, 2, 128), F32),
            pltpu.VMEM((X, 128, 128), BF16),
            pltpu.VMEM((8, 128), jnp.int32),
            pltpu.VMEM((2, NDOC, 128), jnp.int32),
            pltpu.VMEM((8, 128), F32),
            dma((len(inputs),)),
            dma((X,)), dma((X,)),
            dma((2, Z)), dma((2, Z)),
            dma((2, 2, 4)), dma((2, 2, 4)),
            dma((2, 4)), dma((2, 4)),
            dma((2, X)), dma((2, X)),
            dma((Y,)), dma((Y,)),
            dma((2, Y)), dma((2, Y)),
            dma((X,)), dma((X,)),
        ],
        compiler_params=pltpu.CompilerParams(
            collective_id=0, has_side_effects=True, vmem_limit_bytes=56 * 2**20,
        ),
    )(tokens, doc_lengths, *inputs[1:])
    return pl.pallas_call(
        finish,
        out_shape=(
            jax.ShapeDtypeStruct((128, output_weight.shape[1]), BF16),
            jax.ShapeDtypeStruct((2, 128), F32),
        ),
        in_specs=[vm, vm],
        out_specs=(hbm, hbm),
        scratch_shapes=[dma((2,))],
        compiler_params=pltpu.CompilerParams(vmem_limit_bytes=2**20),
    )(*(pltpu.with_memory_space_constraint(a, pltpu.VMEM) for a in results))


def solution(mesh):
    split = split_of(mesh.shape["sp"])
    return jax.shard_map(
        functools.partial(per_device, split, mesh.shape["tp"]),
        mesh=mesh,
        in_specs=(
            P(("sp", "tp"), None),
            P(), P(), P(), P(), P(), P(),
            P(None, "tp"), P(None, "tp"), P(None, "tp"),
            P(), P(), P(),
            P(None, "tp"),
        ),
        out_specs=(P("sp", "tp"), P("tp", "sp")),
        check_vma=False,
    )
```

```python
import functools

import jax
import jax.numpy as jnp
import numpy as np
from jax import lax
from jax.experimental import pallas as pl
from jax.experimental.pallas import tpu as pltpu
from jax.sharding import PartitionSpec as P

NOPE = 64
ROPE = 32
VD = 64
NDOC = 16
WIDTH = NOPE + ROPE
EPS = 1e-06
THETA = 10000.0
APART = -float(2**20)
SCALE = WIDTH**-0.5
LOG2E = 1.4426950408889634
F32 = jnp.float32
BF16 = jnp.bfloat16
MESH = pl.DeviceIdType.MESH
DOC_LANE = 64


def split_of(count):
    return {128: (8, 8, 2), 8: (2, 2, 2), 16: (2, 4, 2)}[count]


def tables(blocks):
    half = ROPE // 2
    inverse = THETA ** (-(np.arange(128) % half).astype(np.float64) / half)
    fine = np.arange(128)[:, None] * inverse[None]
    coarse = (np.arange(blocks) * 128)[:, None] * inverse[None]
    fine = np.stack([np.cos(fine), np.sin(fine)]).astype(np.float32)
    coarse = np.stack([np.cos(coarse), np.sin(coarse)]).astype(np.float32)
    return fine, coarse


def query_rows():
    out = np.zeros((256, 2 * WIDTH), np.float32)
    for j in range(128):
        out[j, (j // 64) * WIDTH + j % 64] = 1
    for j in range(64):
        head, entry = j // 32, j % 32
        out[128 + j, head * WIDTH + NOPE + entry] = 1
        out[192 + j, head * WIDTH + NOPE + (entry + 16) % 32] = 1
    return out


def rope_spread():
    out = np.zeros((128, 1024), np.float32)
    for g in range(4):
        for j in range(64):
            out[32 * g + j % 32, 256 * g + j] = 1
            out[32 * g + (j % 32 + 16) % 32, 256 * g + 128 + j] = 1
    return out


def sum_matrix():
    out = np.zeros((256, 256), np.float32)
    for col in range(256):
        head = col // 64 if col < 128 else ((col - 128) // 32) % 2
        for i in range(128):
            out[i, col] = i // 64 == head
        out[128:160, col] = 1
    return out


def dot(a, b):
    return jnp.dot(a, b, preferred_element_type=F32)


def dot_t(a, b):
    return lax.dot_general(a, b, (((1,), (1,)), ((), ())), preferred_element_type=F32)


def lanes(rows, width=128):
    return lax.broadcasted_iota(jnp.int32, (rows, width), 1)


def rows_of(rows, width=128):
    return lax.broadcasted_iota(jnp.int32, (rows, width), 0)


def head_sums(squares, matrix):
    high = squares.astype(BF16)
    low = (squares - high.astype(F32)).astype(BF16)
    return dot(high, matrix) + dot(low, matrix)


def tiles(Z, Y):
    if (Z, Y) == (8, 8):
        keys = [(i, 0) for i in range(8)]
        queries = [(0, 4), (0, -3), (0, 3), (0, -2), (0, 2), (0, -1), (0, 1), (0, 0)]
        batches = [(0, 1), (1, 3), (4, 2), (6, 2)]
    else:
        keys = [(i, 0) for i in range(Z)]
        queries = [(0, i) for i in range(Y - 1, -1, -1)]
        batches = [(0, 1), (1, Z - 1)]
    return keys, queries, batches


def finish(out, logs, out_h, logs_h, sems):
    copies = [pltpu.make_async_copy(out, out_h, sems.at[0]), pltpu.make_async_copy(logs, logs_h, sems.at[1])]
    for copy in copies:
        copy.start()
    for copy in copies:
        copy.wait()


def gain_columns():
    out = np.zeros((WIDTH, 384), np.float32)
    for j in range(128):
        entry = j % 32
        out[j % 64, j] = 1
        out[NOPE + entry, 128 + j] = 1
        out[NOPE + (entry + 16) % 32, 256 + j] = -1 if entry < 16 else 1
    return out


def kernel(
    Z, Y, C, X, keys, queries, batches,
    tok_h, doclen, qdown_h, ldown_h, rdown_h, qlgain_h, lgain_h, qup_h, kup_h, vup_h, qgain_h, kgain_h, ogain_h, oweight_h,
    fine_h, coarse_h, qcols_h, spread_h, ksum_h, gcols_h,
    out, logs,
    tok, qdown, ldown, rdown, qlgain, lgain, qup, kup, vup, qgain, kgain, ogain, oweight,
    fine, coarse, qcols, spread, ksum, gcols,
    qlbuf, klbuf, rkbuf, qbuf, kall, vtall, sbuf0, sbuf1, pbuf0, pbuf1, stats, qside, qtable, vupt, osend, lsend, orecv, lrecv, hobuf, bounds, columns, gains,
    in_s, ql_s, ql_r, kz_s, kz_r, kx_s, kx_r, kf_s, kf_r, kc_s, kc_r, qy_s, qy_r, o_s, o_r, ho_s, ho_r,
):
    s = lax.axis_index("sp")
    t = lax.axis_index("tp")
    z = s // (Y * C)
    y = lax.rem(s // C, Y)
    c = lax.rem(s, C)
    gz = len(keys) * 32
    groups = C * X
    blocks = len(queries)
    side = 1 - 2 * c

    def at(zz, yy, cc):
        return (zz * Y + yy) * C + cc

    def chip(dz, dy):
        return lax.rem(z + dz + 2 * Z, Z), lax.rem(y + dy + 2 * Y, Y)

    def kpeer(i, way):
        return at(*chip(way * keys[i][0], way * keys[i][1]), c), t

    def picked(i, which):
        if isinstance(i, int):
            return queries[i][which]
        out = jnp.int32(0)
        for n, step in enumerate(queries):
            out = jnp.where(i == n, step[which], out)
        return out

    def qblock(i, way):
        return at(*chip(way * side * picked(i, 0), way * side * picked(i, 1)), c)

    def qpeer(i, way):
        return qblock(i, way), t

    def xof(k):
        return lax.rem(t + k + X, X)

    def xpeer(k):
        return s, xof(k)

    other = (at(z, y, 1 - c), t)

    def remote(src, dst, ss, rs, who):
        return pltpu.make_async_remote_copy(
            src_ref=src, dst_ref=dst, send_sem=ss, recv_sem=rs, device_id=who, device_id_type=MESH
        )

    pairs = [
        (tok_h, tok), (ldown_h, ldown), (lgain_h, lgain), (rdown_h, rdown), (qdown_h, qdown), (qlgain_h, qlgain),
        (qup_h, qup), (qcols_h, qcols), (qgain_h, qgain), (kgain_h, kgain), (gcols_h, gcols), (vup_h, vup),
        (fine_h, fine), (coarse_h, coarse), (kup_h, kup), (spread_h, spread), (ksum_h, ksum),
        (ogain_h, ogain), (oweight_h, oweight),
    ]
    loads = [pltpu.make_async_copy(a, b, in_s.at[i]) for i, (a, b) in enumerate(pairs)]
    for load in loads[:4]:
        load.start()
    barrier = pltpu.get_barrier_semaphore()
    near = {(w * dz % Z, w * dy % Y) for dz, dy in queries[:-1] for w in (1, -1)}
    peers = [(at(*chip(dz, dy), c), t) for dz, dy in sorted(near | set(keys[1:]))]
    peers += [xpeer(k) for k in range(1, X)] + [other]
    for who in peers:
        pl.semaphore_signal(barrier, inc=1, device_id=who, device_id_type=MESH)

    sends = []

    def post(copy):
        copy.start()
        sends.append(copy)

    for load in loads[0:4]:
        load.wait()
    for load in loads[4:]:
        load.start()
    x = tok[...]
    kd = dot(x, ldown[...])
    kd = kd * lax.rsqrt(jnp.mean(kd * kd, axis=-1, keepdims=True) + EPS) * lgain[...]
    klbuf[t, 0] = kd.astype(BF16)
    rope = rdown[...]
    rk4 = dot_t(x, jnp.concatenate([rope, rope, rope, rope], axis=0)).astype(BF16).astype(F32)
    group = lanes(8) // 32
    rkbuf[t, 0] = jnp.where(
        group == 0, rk4[0:8], jnp.where(group == 1, rk4[8:16], jnp.where(group == 2, rk4[16:24], rk4[24:32]))
    ).astype(BF16)

    pl.semaphore_wait(barrier, len(peers))

    for i in range(len(keys) - 1, 0, -1):
        for n, buf in enumerate((klbuf, rkbuf)):
            post(remote(buf.at[t, 0], buf.at[t, i], kz_s.at[n, i], kz_r.at[n, i], kpeer(i, -1)))

    def to_x(i):
        first, count = batches[i]
        for n, buf in enumerate((klbuf, rkbuf)):
            part = buf.at[t, pl.ds(first, count)]
            for d in range(2):
                post(remote(part, part, kx_s.at[n, d, i], kx_r.at[n, d, i], xpeer(1 - 2 * d)))

    to_x(0)

    for load in loads[4:6]:
        load.wait()
    qd = dot(tok[...], qdown[...])
    qd = qd * lax.rsqrt(jnp.mean(qd * qd, axis=-1, keepdims=True) + EPS) * qlgain[...]
    qlbuf[t] = qd.astype(BF16)
    for k in range(1, X):
        post(remote(qlbuf.at[t], qlbuf.at[t], ql_s.at[k], ql_r.at[k], xpeer(k)))

    def from_z(i):
        first, count = batches[i]
        for slot in range(first, first + count):
            for n, buf in enumerate((klbuf, rkbuf)):
                remote(buf.at[t, 0], buf.at[t, slot], kz_s.at[n, slot], kz_r.at[n, slot], kpeer(slot, 1)).wait_recv()
        to_x(i)

    for load in loads[6:]:
        load.wait()
    lane1 = lanes(1)
    starts = jnp.full((1, 128), 1 << 30, jnp.int32)
    ends = jnp.zeros((1, 128), jnp.int32)
    total = jnp.int32(0)
    for d in range(NDOC):
        starts = jnp.where(lane1 == DOC_LANE + d, total, starts)
        total = total + doclen[d]
        ends = jnp.where(lane1 == DOC_LANE + d, total, ends)
    bounds[0:1, :] = starts
    bounds[1:2, :] = ends
    which = rows_of(NDOC)
    total = jnp.int32(0)
    starts = jnp.zeros((NDOC, 128), jnp.int32)
    ends = jnp.zeros((NDOC, 128), jnp.int32)
    for d in range(NDOC):
        starts = jnp.where(which == d, total, starts)
        total = total + doclen[d]
        ends = jnp.where(which == d, total, ends)
    columns[0] = starts
    columns[1] = ends
    for n, gain in enumerate((qgain, kgain)):
        high = gain[...].astype(BF16)
        rest = gain[...] - high.astype(F32)
        middle = rest.astype(BF16)
        low = (rest - middle.astype(F32)).astype(BF16)
        spots = sum(dot(jnp.broadcast_to(piece, (8, WIDTH)), gcols[...]) for piece in (high, middle, low))
        for i in range(3):
            gains[3 * n + i : 3 * n + i + 1, :] = spots[0:1, 128 * i : 128 * i + 128]
    qweight = dot(qcols[...], qup[...]).astype(BF16)
    vupt[...] = jnp.transpose(vup[...].astype(F32)).astype(BF16)

    def turn(block, first, count):
        cb = coarse[0, pl.ds(block, 1), :]
        sb = coarse[1, pl.ds(block, 1), :]
        cf = fine[0, pl.ds(first, count), :]
        sf = fine[1, pl.ds(first, count), :]
        return cb * cf - sb * sf, sb * cf + cb * sf

    cosine, sine = turn(s, 0, 128)
    qtable[0:64, :] = jnp.transpose(cosine * gains[1:2, :])[0:64, :]
    qtable[64:128, :] = jnp.transpose(sine * gains[2:3, :])[0:64, :]
    qtable[128:256, :] = jnp.transpose(jnp.broadcast_to(gains[0:1, :], (128, 128)))
    qside[...] = jnp.zeros((256, 256), BF16)

    from_z(1)
    for k in range(1, X):
        xx = xof(-k)
        remote(qlbuf.at[xx], qlbuf.at[xx], ql_s.at[k], ql_r.at[k], (s, xx)).wait_recv()
    qq = dot_t(qweight, qlbuf[...].reshape(128, qlbuf.shape[2]))
    for h in range(2):
        q0 = qq[64 * h : 64 * h + 64]
        q1 = qq[128 + 32 * h : 160 + 32 * h]
        q2 = qq[192 + 32 * h : 224 + 32 * h]
        qs = jnp.sum(q0 * q0, axis=0, keepdims=True) + jnp.sum(q1 * q1, axis=0, keepdims=True)
        qs = lax.rsqrt(qs * (1.0 / WIDTH) + EPS)
        qbuf[blocks - 1, 64 * h : 64 * h + 64, :] = (q0 * qs * qtable[128 + 64 * h : 192 + 64 * h, :]).astype(BF16)
        turned = q1 * qtable[32 * h : 32 * h + 32, :] + q2 * qtable[64 + 32 * h : 96 + 32 * h, :]
        qbuf[blocks - 1, 128 + 32 * h : 160 + 32 * h, :] = (turned * qs).astype(BF16)
    for i in range(blocks - 1):
        post(remote(qbuf.at[blocks - 1], qbuf.at[i], qy_s.at[i], qy_r.at[i], qpeer(i, -1)))

    for i in range(2, len(batches)):
        from_z(i)

    def expand(xx):
        kl = klbuf[xx].reshape(gz, klbuf.shape[3])
        index = c * X + xx
        vtall[index] = dot_t(vupt[...], kl).astype(BF16)
        raw = dot(kl, kup[...])
        spreaded = dot(rkbuf[xx].astype(F32).reshape(gz // 4, 128).astype(BF16), spread[...])

        def rows_from(shift):
            return jnp.concatenate(
                [spreaded[8 * i : 8 * i + 8, 256 * g + shift : 256 * g + shift + 128] for i in range(len(keys)) for g in range(4)],
                axis=0,
            )

        r1, r2 = rows_from(0), rows_from(128)
        sums = head_sums(jnp.concatenate([raw * raw, r1 * r1], axis=1), ksum[...])
        sums = lax.rsqrt(sums * (1.0 / WIDTH) + EPS)
        kall[index, :, 0:128] = (raw * sums[:, 0:128] * gains[3:4, :]).astype(BF16)
        first = pl.multiple_of(xx * 32, 32)
        for i in range(len(keys)):
            block = at(*chip(*keys[i]), c)
            cosine, sine = turn(block, first, 32)
            part = slice(i * 32, i * 32 + 32)
            turned = (r1[part] * gains[4:5, :] * cosine + r2[part] * gains[5:6, :] * sine) * sums[part, 128:256]
            place = block * 128 + first + rows_of(32)
            inside = (place >= bounds[0:1, :]) & (place < bounds[1:2, :])
            kall[index, part, 128:256] = jnp.where(inside, 1.0, turned).astype(BF16)

    def to_core(xx):
        index = c * X + xx
        for n, buf in enumerate((kall, vtall)):
            post(remote(buf.at[index], buf.at[index], kc_s.at[n, xx], kc_r.at[n, xx], other))

    expand(t)
    for i, (first, count) in enumerate(batches):
        for d in range(2):
            xx = xof(2 * d - 1)
            for n, buf in enumerate((klbuf, rkbuf)):
                part = buf.at[xx, pl.ds(first, count)]
                remote(part, part, kx_s.at[n, d, i], kx_r.at[n, d, i], (s, xx)).wait_recv()
                if d == onward(i):
                    post(remote(part, part, kf_s.at[n, i], kf_r.at[n, i], xpeer(1 - 2 * d)))
    to_core(t)
    expand(xof(-1))
    expand(xof(1))
    for i, (first, count) in enumerate(batches):
        xx = xof(2)
        for n, buf in enumerate((klbuf, rkbuf)):
            part = buf.at[xx, pl.ds(first, count)]
            remote(part, part, kf_s.at[n, i], kf_r.at[n, i], xpeer(2 * onward(i) - 1)).wait_recv()
    to_core(xof(-1))
    to_core(xof(1))
    expand(xof(2))
    to_core(xof(2))
    for xx in range(X):
        index = (1 - c) * X + xx
        for n, buf in enumerate((kall, vtall)):
            remote(buf.at[index], buf.at[index], kc_s.at[n, xx], kc_r.at[n, xx], other).wait_recv()

    sbufs, pbufs = (sbuf0, sbuf1), (pbuf0, pbuf1)

    def prepare(i):
        place = qblock(i, 1) * 128 + lanes(NDOC)
        inside = (place >= columns[0]) & (place < columns[1])
        apart = jnp.where(inside, 0.0, APART).astype(BF16)
        for h in range(2):
            cols = slice(128 * h, 128 * h + 128)
            qside[64 * h : 64 * h + 64, cols] = qbuf[i, 64 * h : 64 * h + 64, :]
            qside[128 + 32 * h : 160 + 32 * h, cols] = qbuf[i, 128 + 32 * h : 160 + 32 * h, :]
            qside[128 + DOC_LANE : 128 + DOC_LANE + NDOC, cols] = apart
    def score(par, g, most):
        scores = dot(kall[g], qside[...])
        for r in range(gz // 8):
            part = scores[8 * r : 8 * r + 8]
            sbufs[par][g, 8 * r : 8 * r + 8, :] = part
            most[r % 2] = part if most[r % 2] is None else jnp.maximum(most[r % 2], part)

    def scored(par, most):
        top = jnp.max(jnp.maximum(most[0], most[1]), axis=0, keepdims=True)
        stats[par] = jnp.broadcast_to(top, (8, 256)) * (SCALE * LOG2E)

    def weigh(par, g, count):
        top = stats[par]
        for r in range(gz // 16):
            rows = slice(16 * r, 16 * r + 16)
            weights = [
                jnp.exp2(sbufs[par][g, 16 * r + o : 16 * r + o + 8, :] * (SCALE * LOG2E) - top) for o in (0, 8)
            ]
            pbufs[par][g, rows, :] = jnp.concatenate(weights, axis=0).astype(BF16)
            for o in range(2):
                count[o] = weights[o] if count[o] is None else count[o] + weights[o]

    def weighed(par, count):
        stats[2 + par] = jnp.broadcast_to(jnp.sum(count[0] + count[1], axis=0, keepdims=True), (8, 256))
        stats[4 + par] = stats[par] * (1.0 / LOG2E)

    def gather(par, g, accs):
        update = dot(vtall[g], pbufs[par][g])
        accs[g % 2] = update if accs[g % 2] is None else accs[g % 2] + update

    def gathered(i, par, accs):
        acc = accs[0] + accs[1]
        top, count = stats[4 + par, 0:1, :], stats[2 + par, 0:1, :]
        log = top + jnp.log(count)
        lsend[i] = jnp.where(rows_of(2) == 0, log[:, 0:128], log[:, 128:256])
        inv = 1.0 / count
        osend[i, 0:64, :] = (acc[0:64, 0:128] * inv[:, 0:128]).astype(BF16)
        osend[i, 64:128, :] = (acc[64:128, 128:256] * inv[:, 128:256]).astype(BF16)

    def work(i, par, first, second, third):
        most, count, accs = [None, None], [None, None], [None, None]
        if first:
            prepare(i)
        for g in range(groups):
            if third:
                gather(par, g, accs)
            if first:
                score(par, g, most)
            if second:
                weigh(1 - par, g, count)
        if third:
            gathered(i - 2, par, accs)
        if first:
            scored(par, most)
        if second:
            weighed(1 - par, count)

    def receive(i):
        remote(qbuf.at[blocks - 1], qbuf.at[i], qy_s.at[i], qy_r.at[i], qpeer(i, 1)).wait_recv()

    def results(i, way):
        who = qpeer(i, way)
        return (
            remote(osend.at[i], orecv.at[i], o_s.at[0, i], o_r.at[0, i], who),
            remote(lsend.at[i], lrecv.at[i], o_s.at[1, i], o_r.at[1, i], who),
        )

    def give(i):
        for copy in results(i, 1):
            copy.start()

    receive(jnp.int32(0))
    work(jnp.int32(0), 0, True, False, False)
    work(jnp.int32(1), 1, False, True, False)
    work(jnp.int32(2), 0, False, False, True)
    give(jnp.int32(0))
    if blocks > 2:
        receive(jnp.int32(1))
    work(jnp.int32(1), 1, True, False, False)
    if blocks == 2:
        work(jnp.int32(2), 0, False, True, False)
        work(jnp.int32(3), 1, False, False, True)
    else:
        receive(jnp.int32(2))
        work(jnp.int32(2), 0, True, True, False)

        def step(pair, carry):
            for n in range(2):
                i = 3 + 2 * pair + n
                receive(i)
                work(i, 1 - n, True, True, True)
                give(i - 2)
            return carry

        lax.fori_loop(0, (blocks - 4) // 2, step, 0)
        work(jnp.int32(blocks - 1), 1, True, True, True)
        give(jnp.int32(blocks - 3))
        work(jnp.int32(blocks), 0, False, True, True)
        give(jnp.int32(blocks - 2))
        work(jnp.int32(blocks + 1), 1, False, False, True)

    own = blocks - 1
    orecv[own] = osend[own]
    lrecv[own] = lsend[own]
    for i in range(own):
        for copy in results(i, -1):
            copy.wait_recv()
    top = lrecv[0]
    for i in range(1, blocks):
        top = jnp.maximum(top, lrecv[i])
    whole = jnp.zeros_like(top)
    acc0 = jnp.zeros((64, 128), F32)
    acc1 = jnp.zeros((64, 128), F32)
    for i in range(blocks):
        weight = jnp.exp(lrecv[i] - top)
        whole = whole + weight
        acc0 = acc0 + weight[0:1] * orecv[i, 0:64, :].astype(F32)
        acc1 = acc1 + weight[1:2] * orecv[i, 64:128, :].astype(F32)
    logs[...] = top + jnp.log(whole)
    inv = 1.0 / whole
    heads = jnp.concatenate([acc0 * inv[0:1], acc1 * inv[1:2]], axis=0)
    hobuf[t] = jnp.transpose(heads).astype(BF16)
    for k in range(1, X):
        post(remote(hobuf.at[t], hobuf.at[t], ho_s.at[k], ho_r.at[k], xpeer(k)))
    for i in range(own):
        for copy in results(i, 1):
            copy.wait_send()
    for k in range(1, X):
        xx = xof(-k)
        remote(hobuf.at[xx], hobuf.at[xx], ho_s.at[k], ho_r.at[k], (s, xx)).wait_recv()
    full = jnp.concatenate([hobuf[i].astype(F32) for i in range(X)], axis=1)
    normed = full * lax.rsqrt(jnp.mean(full * full, axis=-1, keepdims=True) + EPS) * ogain[...]
    out[...] = dot(normed.astype(BF16), oweight[...]).astype(BF16)
    for copy in sends:
        copy.wait_send()


def onward(batch):
    return (0, 1, 0, 1)[batch]


def per_device(
    split, X,
    tokens, doc_lengths, query_down, latent_down, rope_down, query_latent_gain, latent_gain,
    query_up, key_up, value_up, query_gain, key_gain, output_gain, output_weight,
):
    Z, Y, C = split
    fine, coarse = tables(Z * Y * C)
    hbm = pl.BlockSpec(memory_space=pltpu.HBM)
    vm = pl.BlockSpec(memory_space=pltpu.VMEM)
    sm = pl.BlockSpec(memory_space=pltpu.SMEM)
    dma = pltpu.SemaphoreType.DMA
    keys, queries, batches = tiles(Z, Y)
    gz = len(keys) * 32
    groups = C * X
    Y, Z = len(queries), len(keys)
    QR, KVR = query_down.shape[1], latent_down.shape[1]
    const = lambda a: jnp.asarray(a, BF16)
    row = lambda a: a.reshape(1, -1)
    inputs = [
        tokens, query_down, latent_down, rope_down.T, row(query_latent_gain), row(latent_gain),
        query_up.T, key_up, value_up, row(query_gain), row(key_gain), row(output_gain), output_weight,
        jnp.asarray(fine), jnp.asarray(coarse), const(query_rows()), const(rope_spread()),
        const(sum_matrix()), const(gain_columns()),
    ]
    results = pl.pallas_call(
        functools.partial(kernel, *split, X, keys, queries, batches),
        out_shape=(
            pltpu.VMEM((128, output_weight.shape[1]), BF16),
            pltpu.VMEM((2, 128), F32),
        ),
        in_specs=[hbm, sm] + [hbm] * (len(inputs) - 1),
        out_specs=(vm, vm),
        scratch_shapes=[pltpu.VMEM(a.shape, a.dtype) for a in inputs] + [
            pltpu.VMEM((X, 32, QR), BF16),
            pltpu.VMEM((X, Z, 32, KVR), BF16),
            pltpu.VMEM((X, Z, 8, 128), BF16),
            pltpu.VMEM((Y, 192, 128), BF16),
            pltpu.VMEM((groups, gz, 256), BF16),
            pltpu.VMEM((groups, 128, gz), BF16),
            pltpu.VMEM((groups, gz, 256), F32),
            pltpu.VMEM((groups, gz, 256), F32),
            pltpu.VMEM((groups, gz, 256), BF16),
            pltpu.VMEM((groups, gz, 256), BF16),
            pltpu.VMEM((6, 8, 256), F32),
            pltpu.VMEM((256, 256), BF16),
            pltpu.VMEM((256, 128), F32),
            pltpu.VMEM((128, KVR), BF16),
            pltpu.VMEM((Y, 128, 128), BF16),
            pltpu.VMEM((Y, 2, 128), F32),
            pltpu.VMEM((Y, 128, 128), BF16),
            pltpu.VMEM((Y, 2, 128), F32),
            pltpu.VMEM((X, 128, 128), BF16),
            pltpu.VMEM((8, 128), jnp.int32),
            pltpu.VMEM((2, NDOC, 128), jnp.int32),
            pltpu.VMEM((8, 128), F32),
            dma((len(inputs),)),
            dma((X,)), dma((X,)),
            dma((2, Z)), dma((2, Z)),
            dma((2, 2, 4)), dma((2, 2, 4)),
            dma((2, 4)), dma((2, 4)),
            dma((2, X)), dma((2, X)),
            dma((Y,)), dma((Y,)),
            dma((2, Y)), dma((2, Y)),
            dma((X,)), dma((X,)),
        ],
        compiler_params=pltpu.CompilerParams(
            collective_id=0, has_side_effects=True, vmem_limit_bytes=56 * 2**20,
        ),
    )(tokens, doc_lengths, *inputs[1:])
    return pl.pallas_call(
        finish,
        out_shape=(
            jax.ShapeDtypeStruct((128, output_weight.shape[1]), BF16),
            jax.ShapeDtypeStruct((2, 128), F32),
        ),
        in_specs=[vm, vm],
        out_specs=(hbm, hbm),
        scratch_shapes=[dma((2,))],
        compiler_params=pltpu.CompilerParams(vmem_limit_bytes=2**20),
    )(*(pltpu.with_memory_space_constraint(a, pltpu.VMEM) for a in results))


def solution(mesh):
    split = split_of(mesh.shape["sp"])
    return jax.shard_map(
        functools.partial(per_device, split, mesh.shape["tp"]),
        mesh=mesh,
        in_specs=(
            P(("sp", "tp"), None),
            P(), P(), P(), P(), P(), P(),
            P(None, "tp"), P(None, "tp"), P(None, "tp"),
            P(), P(), P(),
            P(None, "tp"),
        ),
        out_specs=(P("sp", "tp"), P("tp", "sp")),
        check_vma=False,
    )
```
